512 devices in a mesh: kv: 128 (over z, y, core), tp: 4 (over x).
Axes of the slice: x: 4, y: 8, z: 8, core: 2. Of those that a mesh axis runs over, the one named last changes fastest.
Arguments:
- hidden: bfloat16 [128, 4096], P(None, 'tp'), may hold values from -50 to 50
- input_gain: bfloat16 [4096], P('tp'), may hold values from 0.099609375 to 1.8984375
- x_weight: bfloat16 [4096, 8192], P('tp', 'kv'), may hold values from -0.09375 to 0.09375
- z_weight: bfloat16 [4096, 8192], P('tp', 'kv'), may hold values from -0.09375 to 0.09375
- bc_weight: bfloat16 [4096, 8192], P('tp', 'kv'), may hold values from -0.09375 to 0.09375
- dt_weight: bfloat16 [4096, 128], P('tp', 'kv'), may hold values from -0.09375 to 0.09375
- x_kernel: bfloat16 [4, 8192], P(None, 'kv'), may hold values from -3 to 3
- bc_kernel: bfloat16 [4, 8192], P(None, 'kv'), may hold values from -3 to 3
- dt_bias: float32 [128], P('kv'), may hold values from -3 to 0.5
- decay_log: float32 [128], P('kv'), may hold values from -3 to 1.5
- skip_scale: float32 [128], P('kv'), may hold values from 0.5 to 1.5
- output_gain: bfloat16 [8192], P('kv'), may hold values from 0.099609375 to 1.8984375
- output_weight: bfloat16 [8192, 4096], P('kv'), may hold values from -0.25 to 0.25
- saved_states: float32 [32, 5, 128, 64, 128], P('tp', None, 'kv'), may hold values from -1.8 to 1.8
- x_history: bfloat16 [32, 7, 8192], P('tp', None, 'kv'), may hold values from -6 to 6
- bc_history: bfloat16 [32, 7, 8192], P('tp', None, 'kv'), may hold values from -6 to 6
- accepted: int32 [32], P('tp'), may hold values from 0 to 4
Outputs:
- mixed: bfloat16 [128, 4096], P('tp', 'kv')
- new_states: float32 [32, 5, 128, 64, 128], P('tp', None, 'kv')
- x_window: bfloat16 [32, 7, 8192], P('tp', None, 'kv')
- bc_window: bfloat16 [32, 7, 8192], P('tp', None, 'kv')
The draws below stay inside these ranges and needn't reach their ends.
All inputs are finite; a program needn't handle non-finite values.
Results may differ from the reference program's by a relative error of at most 0.02.
Values may be sent and summed in bfloat16 or wider, within the bound.
No kernel may reach another device: no remote copies, remote signals or barrier semaphores. Data moves between devices by JAX's collectives and lax.ppermute only.
A program may use at most 64 MiB of HBM per device.

```python
import jax
import jax.numpy as jnp
from jax import lax

D = 4096
HEADS = 128
HEAD_SIZE = 64
STATE = 128
GROUPS = 32
CONV = 4
PROPS = 4
SEQS = 32
TOKENS = 128
INNER = 8192
BC_WIDTH = 8192
HIST = 7
FEATURE_BLOCKS = 4


def draw_hidden(key, part):
    noise_key = jax.random.fold_in(key, 0)
    samples = jnp.clip(jax.random.normal(noise_key, (TOKENS, D), jnp.float32), -6.0, 6.0)
    quarter = jnp.arange(D) * 4 // D
    factors = jnp.array([0.5, 1.6, 0.4, 1.2], jnp.float32)[quarter]
    return (samples * factors[None, :]).astype(jnp.bfloat16)


def set_ends(result, rng, smallest, top_value):
    longest = result.shape.index(max(result.shape))
    spots = []
    for shift in (0, 1):
        where = [jax.random.randint(jax.random.fold_in(rng, axis), (), 0, length) for axis, length in enumerate(result.shape)]
        where[longest] = (where[longest] + shift) % result.shape[longest]
        spots.append(tuple(where))
    return result.at[spots[0]].set(smallest).at[spots[1]].set(top_value)


def with_spikes(entries, rng, source, target, shards_of, factor):
    owner, partner = [(jnp.arange(entries.shape[dim]) // (entries.shape[dim] // shards_of)).reshape([-1 if axis == dim else 1 for axis in range(entries.ndim)]) for dim in (source, target)]
    chosen = jax.random.permutation(rng, shards_of)[partner]
    strong = (owner == chosen) | (owner == (partner + shards_of // 2) % shards_of)
    return jnp.where(strong, factor * entries, entries)


def level_of(rng, extent, shards, low, top_value):
    gain = 1.0
    for axis_at, blocks in shards:
        draws = jax.random.uniform(jax.random.fold_in(jax.random.fold_in(rng, 6), axis_at), (blocks,), jnp.float32, low / len(shards), top_value / len(shards))
        gain = gain * jnp.repeat(jnp.exp(draws), extent[axis_at] // blocks).reshape((-1,) + (1,) * (len(extent) - 1 - axis_at))
    return gain


def bell_draw(key, dims, width, limit, cuts=(), kind=jnp.bfloat16):
    gain = level_of(key, dims, cuts, -0.22, 0.18) if cuts else 1.0
    values = jax.random.normal(key, dims, jnp.float32) * width * gain
    return jnp.minimum(jnp.maximum(values, -limit), limit).astype(kind)


def noise_with(stream_key, extent, spread, reach, cuts, heavy, kind=jnp.bfloat16):
    result = spread * jax.random.normal(stream_key, extent, jnp.float32)
    if cuts:
        result = result * level_of(stream_key, extent, cuts, -0.22, 0.18)
    return jnp.clip(with_spikes(result, jax.random.fold_in(stream_key, 3), *heavy), -reach, reach).astype(kind)


def setup_inputs(seed: int = 0) -> dict:
    streams_of = jax.random.split(jax.random.key(seed), 18)
    return {
        "hidden": draw_hidden(jax.random.fold_in(streams_of[17], 71), 0),
        "input_gain": jnp.clip(1.0 + 0.18 * jax.random.normal(streams_of[1], (D,), jnp.float32), 0.099609375, 1.8984375).astype(jnp.bfloat16),
        "x_weight": bell_draw(streams_of[2], (D, INNER), D ** -0.5, 0.09375, ((0, 4), (1, 128))),
        "z_weight": bell_draw(streams_of[3], (D, INNER), D ** -0.5, 0.09375, ((0, 4), (1, 128))),
        "bc_weight": bell_draw(streams_of[4], (D, BC_WIDTH), D ** -0.5, 0.09375, ((0, 4), (1, 128))),
        "dt_weight": bell_draw(streams_of[5], (D, HEADS), D ** -0.5, 0.09375, ((0, 4), (1, 128))),
        "x_kernel": bell_draw(streams_of[6], (CONV, INNER), CONV ** -0.5, 3.0, ((1, 128),)),
        "bc_kernel": bell_draw(streams_of[7], (CONV, BC_WIDTH), CONV ** -0.5, 3.0, ((1, 128),)),
        "dt_bias": jnp.clip(-3.0 + 3.5 * jax.random.uniform(streams_of[8], (HEADS,), jnp.float32) ** level_of(streams_of[8], (HEADS,), ((0, 128),), -0.2, 0.2), -3.0, 0.5),
        "decay_log": jnp.clip(-3.0 + 4.5 * jax.random.uniform(streams_of[9], (HEADS,), jnp.float32) ** level_of(streams_of[9], (HEADS,), ((0, 128),), -0.2, 0.2), -3.0, 1.5),
        "skip_scale": jnp.clip(0.5 + 1.0 * jax.random.uniform(streams_of[10], (HEADS,), jnp.float32) ** level_of(streams_of[10], (HEADS,), ((0, 128),), -0.2, 0.2), 0.5, 1.5),
        "output_gain": jnp.clip(1.0 + 0.18 * jax.random.normal(streams_of[11], (INNER,), jnp.float32), 0.099609375, 1.8984375).astype(jnp.bfloat16),
        "output_weight": noise_with(streams_of[12], (INNER, D), INNER ** -0.5, 0.25, ((0, 128),), (0, 1, 128, 5.5)),
        "saved_states": bell_draw(streams_of[13], (SEQS, PROPS + 1, HEADS, HEAD_SIZE, STATE), 0.3, 1.8, ((0, 4), (2, 128)), jnp.float32),
        "x_history": bell_draw(streams_of[14], (SEQS, HIST, INNER), 1.0, 6.0, ((0, 4), (2, 128))),
        "bc_history": bell_draw(streams_of[15], (SEQS, HIST, BC_WIDTH), 1.0, 6.0, ((0, 4), (2, 128))),
        "accepted": set_ends(jax.random.randint(streams_of[16], (SEQS,), 0, PROPS + 1), jax.random.fold_in(streams_of[16], 1), 0, PROPS).astype(jnp.int32),
    }


EPSILON = 1e-05

def take_window(history, accepted, fresh_rows):
    history_len = history.shape[1] - fresh_rows.shape[1]
    indices = accepted[:, None] + jnp.arange(history_len, dtype=jnp.int32)[None, :]
    kept_rows = jnp.take_along_axis(history, indices[:, :, None], axis=1)
    return jnp.concatenate([kept_rows, fresh_rows], axis=1)

def conv_silu(window, kernel):
    length = window.shape[1] - kernel.shape[0] + 1
    running = window[:, 0:length].astype(jnp.float32) * kernel[0].astype(jnp.float32)
    for offset in range(1, kernel.shape[0]):
        running = running + window[:, offset:offset + length].astype(jnp.float32) * kernel[offset].astype(jnp.float32)
    return jax.nn.silu(running)

def ssd_block(x_conv, step_size, decay_rate, b_terms, c_terms, first_state, skip_scale):
    cumulated = jnp.cumsum(-decay_rate * step_size, axis=1)
    length = x_conv.shape[1]
    indices = jnp.arange(length)
    causal = indices[:, None] >= indices[None, :]
    gaps = cumulated[:, :, None, :] - cumulated[:, None, :, :]
    weights = jnp.exp(jnp.where(causal[None, :, :, None], gaps, -jnp.inf))
    inputs = x_conv * step_size[..., None]
    outer_prod = jnp.einsum('srhp,srhn->srhpn', inputs, b_terms)
    states = jnp.exp(cumulated)[..., None, None] * first_state[:, None] + jnp.einsum('strh,srhpn->sthpn', weights, outer_prod)
    output = jnp.einsum('sthn,sthpn->sthp', c_terms, states) + skip_scale[:, None] * x_conv
    return (output, states)

def reference(hidden, input_gain, x_weight, z_weight, bc_weight, dt_weight, x_kernel, bc_kernel, dt_bias, decay_log, skip_scale, output_gain, output_weight, saved_states, x_history, bc_history, accepted):
    widened = hidden.astype(jnp.float32)
    normed = (widened * lax.rsqrt(lax.optimization_barrier(jnp.mean(widened * widened, axis=1, keepdims=True)) + EPSILON) * input_gain.astype(jnp.float32)).astype(jnp.bfloat16)
    weights = jnp.concatenate([x_weight, z_weight, bc_weight, dt_weight], axis=1)
    feature_block = D // FEATURE_BLOCKS
    running = jnp.zeros((normed.shape[0], weights.shape[1]), jnp.float32)
    for part_index in range(FEATURE_BLOCKS):
        product = jnp.dot(normed[:, part_index * feature_block:(part_index + 1) * feature_block], weights[part_index * feature_block:(part_index + 1) * feature_block], preferred_element_type=jnp.float32)
        running = running + lax.optimization_barrier(product.astype(jnp.bfloat16)).astype(jnp.float32)
    projected = running.astype(jnp.bfloat16)
    x_fresh = projected[:, :INNER]
    z_fresh = projected[:, INNER:2 * INNER]
    bc_fresh = projected[:, 2 * INNER:2 * INNER + BC_WIDTH]
    dt_fresh = projected[:, 2 * INNER + BC_WIDTH:]
    x_window = take_window(x_history, accepted, x_fresh.reshape(SEQS, PROPS, INNER))
    bc_window = take_window(bc_history, accepted, bc_fresh.reshape(SEQS, PROPS, BC_WIDTH))
    x_conv = conv_silu(x_window, x_kernel).reshape(SEQS, PROPS, HEADS, HEAD_SIZE)
    bc_conv = conv_silu(bc_window, bc_kernel).reshape(SEQS, PROPS, GROUPS, 2, STATE)
    b_terms = jnp.repeat(bc_conv[:, :, :, 0], HEADS // GROUPS, axis=2)
    c_terms = jnp.repeat(bc_conv[:, :, :, 1], HEADS // GROUPS, axis=2)
    step_size = jax.nn.softplus(dt_fresh.astype(jnp.float32).reshape(SEQS, PROPS, HEADS) + dt_bias)
    first_state = jnp.take_along_axis(saved_states, accepted[:, None, None, None, None], axis=1)[:, 0]
    decay_rate = jnp.exp(decay_log)

    def one_sequence(pieces):
        x_one, step_one, b_one, c_one, state_one = pieces
        out_one, states_one = ssd_block(x_one[None], step_one[None], decay_rate, b_one[None], c_one[None], state_one[None], skip_scale)
        return (out_one[0], states_one[0])
    output, states = lax.map(one_sequence, (x_conv, step_size, b_terms, c_terms, first_state))
    new_states = jnp.concatenate([first_state[:, None], states], axis=1)
    gate_values = z_fresh.astype(jnp.float32).reshape(SEQS, PROPS, HEADS, HEAD_SIZE)
    gated = (output * jax.nn.silu(gate_values)).reshape(TOKENS, INNER)
    scaled = (gated * output_gain.astype(jnp.float32)).astype(jnp.bfloat16)
    branch = jnp.dot(scaled, output_weight, preferred_element_type=jnp.float32)
    mixed = (lax.rsqrt(lax.optimization_barrier(jnp.mean(gated * gated, axis=1)) + EPSILON)[:, None] * branch).astype(jnp.bfloat16)
    return (mixed, new_states, x_window, bc_window)
```

```python
import jax
import jax.numpy as jnp
from jax import lax
from jax.experimental import pallas as pl
from jax.experimental.pallas import tpu as pltpu
from jax.sharding import Mesh
from jax.sharding import PartitionSpec as P

D = 4096
PROPS = 4
INNER = 8192
KV = ("z", "yh", "yl", "c")
NEAR = ("yl", "c", "tp")
EPSILON = 1e-05
TP = 4
NEAR_KV = 4
KV_SIZE = 128
SEQS = 8
TOKENS = 32
HEAD = 64
STATE = 128
LINES = 10

F32 = jnp.float32
BF16 = jnp.bfloat16


def rounded(value):
    return value.astype(BF16).astype(F32)


def lanes_of(shape):
    return lax.broadcasted_iota(jnp.int32, shape, len(shape) - 1)


def rows_of(shape):
    return lax.broadcasted_iota(jnp.int32, shape, len(shape) - 2)


def dot_nt(a, b):
    return lax.dot_general(a, b, (((1,), (1,)), ((), ())), preferred_element_type=F32)


def silu(v):
    return v / (1.0 + jnp.exp(-v))


def accepted_column(accepted, shape):
    rows = rows_of(shape)
    column = jnp.zeros(shape, jnp.int32)
    for s in range(SEQS):
        column = jnp.where(rows == s, accepted[s], column)
    return column


def kept_rows(history, column):
    whole = [history[i].astype(F32) for i in range(7)]
    kept = []
    for m in range(3):
        row = whole[m]
        for a in range(1, PROPS + 1):
            row = jnp.where(column == a, whole[m + a], row)
        kept.append(row)
    return kept


def project_body(
    accepted, hidden, gain, x_weight, z_weight, bc_weight, dt_weight, bc_history, bc_kernel, message, first, second
):
    widened = hidden[...].astype(F32)
    scaled = (widened * gain[...].astype(F32)[None, :]).astype(BF16)
    squares = jnp.sum(widened * widened, axis=1, keepdims=True)
    dt_rows = jnp.broadcast_to(dt_weight[...], (HEAD, dt_weight.shape[1]))
    first[...] = dot_nt(scaled, jnp.concatenate([x_weight[...], z_weight[...]], axis=0))
    last = dot_nt(scaled, jnp.concatenate([bc_weight[...], dt_rows], axis=0))
    second[...] = last
    turned = jnp.transpose(jnp.where(lanes_of((128, 128)) == HEAD + 1, squares, last))
    dt_line = jnp.broadcast_to(turned[HEAD : HEAD + 1], (8, 128))
    square_line = jnp.broadcast_to(turned[HEAD + 1 : HEAD + 2], (8, 128))
    square_high = rounded(square_line)
    rows = rows_of((8, 128))
    upper = lanes_of((8, 128)) >= HEAD
    lines = jnp.where(rows == 4, dt_line, jnp.where(rows == 5, square_high, square_line - square_high))
    column = accepted_column(accepted, (SEQS, HEAD))
    empty = jnp.zeros((SEQS, HEAD), F32)
    extra = [jnp.concatenate([empty, row], axis=1) for row in kept_rows(bc_history, column)]
    taps = jnp.concatenate([bc_kernel[...].astype(F32), jnp.zeros((4, HEAD), F32)], axis=0)
    taps = jnp.concatenate([empty, taps], axis=1)
    for j in range(TP):
        top = [first[pl.ds(TOKENS * j + t, SEQS, stride=PROPS), :] for t in range(PROPS)]
        low = [second[pl.ds(TOKENS * j + t, SEQS, stride=PROPS), :] for t in range(PROPS)]
        ending = jnp.where(rows < 4, taps, pltpu.roll(lines, (64 - 32 * j) % 128, 1))
        low = [jnp.where(upper, e, v) for e, v in zip([*extra, ending], low)]
        block = jnp.concatenate(top + low, axis=0).astype(BF16)
        for g in range(NEAR_KV):
            message[g * TP + j] = block


def prepare_body(accepted, saved, weight, first_state, turned_weight, arrivals):
    copies = [
        pltpu.make_async_copy(saved.at[s, accepted[s], 0], first_state.at[s], arrivals.at[s]) for s in range(SEQS)
    ]
    for copy in copies:
        copy.start()
    gap = jnp.zeros((LINES - 8, 256), F32)

    def turn(i, _):
        block = weight[:, pl.ds(pl.multiple_of(i * 256, 256), 256)].astype(F32)
        turned = jnp.transpose(block)
        pieces = []
        for d in range(8):
            quarter = [turned[32 * d + 8 * q : 32 * d + 8 * q + 8] for q in range(4)]
            pieces += [jnp.concatenate(quarter, axis=1), gap]
        turned_weight[pl.ds(pl.multiple_of(i * 8 * LINES, 16), 8 * LINES), :] = jnp.concatenate(pieces, axis=0).astype(
            BF16
        )
        return 0

    lax.fori_loop(0, weight.shape[1] // 256, turn, 0)
    for copy in copies:
        copy.wait()


def mix_body(
    accepted,
    dt_bias,
    decay_log,
    skip_scale,
    arrived,
    first_state,
    turned_weight,
    x_kernel,
    x_history,
    output_gain,
    message,
    x_window,
    bc_window,
    inputs_out,
    b_out,
    decay_out,
    columns,
    ordered,
    square_rows,
):
    place = lax.axis_index(("yl", "c"))
    mine = lax.axis_index("tp")
    tile = (SEQS, 128)
    lanes = lanes_of(tile)
    rows = rows_of(tile)
    lower = lanes < HEAD

    def tiles(value):
        return [value[8 * i : 8 * i + 8] for i in range(value.shape[0] // 8)]

    own = arrived[place * TP].astype(F32)
    for k in range(1, TP):
        own = own + arrived[place * TP + k].astype(F32)
    own = tiles(own)
    ending = own[7]
    mean = (ending[5:6] + ending[6:7]) / D
    lined = jnp.where(rows == 5, jnp.broadcast_to(lax.rsqrt(mean + EPSILON), tile), ending)
    columns[...] = jnp.transpose(lined)[HEAD : HEAD + TOKENS]
    scale, step, cumulated = [], [], []
    rate = jnp.exp(jnp.full((SEQS, 1), decay_log[0], F32))
    total = jnp.zeros((SEQS, 1), F32)
    for t in range(PROPS):
        column = columns[pl.ds(t, SEQS, stride=PROPS), :]
        scale.append(column[:, 5:6])
        raw = rounded(column[:, 5:6] * column[:, 4:5]) + dt_bias[0]
        step.append(jnp.maximum(raw, 0.0) + jnp.log1p(jnp.exp(-jnp.abs(raw))))
        total = total - rate * step[t]
        cumulated.append(total)
    fresh = [rounded(scale[t] * own[t]) for t in range(PROPS)]
    sums, extras = [], []
    for g in range(NEAR_KV):
        group = arrived[g * TP, 32:64, :].astype(F32)
        for k in range(1, TP):
            group = group + arrived[g * TP + k, 32:64, :].astype(F32)
        sums.append(tiles(group))
        extras.append(tiles(arrived[g * TP + mine, 32:64, :].astype(F32)))

    def convolved(window, taps):
        results = []
        for t in range(PROPS):
            running = window[t] * taps[0:1]
            for j in range(1, 4):
                running = running + window[t + j] * taps[j : j + 1]
            results.append(silu(running))
        return results

    def terms(left, right):
        window = [
            jnp.where(lower, pltpu.roll(extras[left][m], HEAD, 1), extras[right][m]) for m in range(4)
        ]
        new = [
            rounded(scale[t] * jnp.where(lower, sums[left][t], pltpu.roll(sums[right][t], HEAD, 1)))
            for t in range(PROPS)
        ]
        return convolved(window[:3] + new, window[3])

    b_terms = terms(0, 1)
    c_terms = terms(2, 3)
    column = accepted_column(accepted, (SEQS, HEAD))
    kept = kept_rows(x_history, column)
    empty = jnp.zeros((SEQS, HEAD), F32)
    x_taps = jnp.concatenate([x_kernel[...].astype(F32), jnp.zeros((4, HEAD), F32)], axis=1)
    x_conv = convolved([jnp.concatenate([row, empty], axis=1) for row in kept] + fresh, x_taps)
    states = first_state[...].reshape(SEQS * HEAD, STATE).astype(BF16)
    read = dot_nt(jnp.concatenate(c_terms, axis=0).astype(BF16), states)
    gain = output_gain[...].astype(F32)
    for t in range(PROPS):
        picked = jnp.zeros(tile, F32)
        for k in range(SEQS // 2):
            picked = jnp.where(rows // 2 == k, read[8 * t : 8 * t + 8, 128 * k : 128 * k + 128], picked)
        picked = jnp.where(rows % 2 == 0, picked, pltpu.roll(picked, HEAD, 1))
        output = jnp.exp(cumulated[t]) * picked
        for r in range(t + 1):
            product = jnp.sum(c_terms[t] * b_terms[r], axis=1, keepdims=True)
            output = output + (jnp.exp(cumulated[t] - cumulated[r]) * step[r] * product) * x_conv[r]
        output = output + skip_scale[0] * x_conv[t]
        gated = jnp.where(lower, output * silu(pltpu.roll(fresh[t], HEAD, 1)), 0.0)
        square = jnp.sum(gated * gated, axis=1, keepdims=True)
        ordered[pl.ds(t, SEQS, stride=PROPS), :] = gated
        square_rows[pl.ds(t, SEQS, stride=PROPS), :] = jnp.broadcast_to(square, tile)
        inputs_out[8 * t : 8 * t + 8, :] = x_conv[t] * step[t]
        b_out[8 * t : 8 * t + 8, :] = b_terms[t]
        decay_out[8 * t : 8 * t + 8, :] = jnp.broadcast_to(jnp.exp(-rate * step[t]), tile)
    scaled = ordered[...] * jnp.concatenate([gain, gain], axis=1)
    scaled = scaled.astype(BF16)
    moved = pltpu.roll(ordered[...], HEAD, 1) * jnp.concatenate([gain, gain], axis=1)
    moved = moved.astype(BF16)
    none = jnp.zeros((TOKENS, 128), BF16)
    spread = jnp.concatenate(
        [
            jnp.concatenate([scaled, none], axis=1),
            jnp.concatenate([moved, none], axis=1),
            jnp.concatenate([none, scaled], axis=1),
            jnp.concatenate([none, moved], axis=1),
        ],
        axis=0,
    )
    squares = square_rows[...]
    square_line = jnp.transpose(jnp.concatenate([squares] * 4, axis=0))[0:1]
    high = rounded(square_line)
    low = square_line - high
    period = 4 * LINES
    spot = rows_of((period, 128)) % LINES
    lines = jnp.where(spot == 8, high, jnp.where(spot == 9, low, 0.0))
    part = 8 * period
    lines = jnp.concatenate([lines] * 8, axis=0)
    for i in range(turned_weight.shape[0] // part):
        product = dot_nt(turned_weight[part * i : part * (i + 1), :], spread)
        message[part * i : part * (i + 1), :] = (product + lines).astype(BF16)
    own_extra = tiles(arrived[place * TP + mine, 32:64, :].astype(F32))
    for m in range(3):
        x_window[m] = kept[m].astype(BF16)
        bc_window[m] = pltpu.roll(own_extra[m], HEAD, 1)[:, :HEAD].astype(BF16)
    for t in range(PROPS):
        x_window[3 + t] = fresh[t][:, :HEAD].astype(BF16)
        bc_window[3 + t] = (scale[t] * own[4 + t])[:, :HEAD].astype(BF16)


def state_body(inputs, b_terms, decay, first_state, new_states):
    padded = jnp.concatenate([inputs[...], jnp.zeros((128 - TOKENS, 128), F32)], axis=0)
    turned = jnp.transpose(padded)[:HEAD]
    for s in range(SEQS):
        state = first_state[s]
        new_states[s, 0, 0] = state
        for t in range(PROPS):
            at = 8 * t + s
            state = state * decay[at : at + 1, :] + turned[:, at : at + 1] * b_terms[at : at + 1, :]
            new_states[s, t + 1, 0] = state


def finish_body(arrived, mixed, total):
    step = 8 * LINES
    running = arrived[0:step, :].astype(F32)
    for i in range(1, arrived.shape[0] // step):
        running = running + arrived[step * i : step * (i + 1), :].astype(F32)
    total[...] = running
    summed = total[0:8, :]
    squares = total[8:10, :]
    for i in range(1, 8):
        summed = summed + total[LINES * i : LINES * i + 8, :]
        squares = squares + total[LINES * i + 8 : LINES * i + 10, :]
    mean = (squares[0:1] + squares[1:2]) / INNER
    summed = summed * lax.rsqrt(mean + EPSILON)
    stacked = jnp.concatenate([summed] + [pltpu.roll(summed, 128 - 32 * q, 1) for q in range(1, 4)], axis=0)
    mixed[...] = jnp.transpose(stacked)[:TOKENS].astype(BF16)


def smem():
    return pl.BlockSpec(memory_space=pltpu.SMEM)


def vmem():
    return pl.BlockSpec(memory_space=pltpu.VMEM)


def local(
    hidden,
    input_gain,
    x_weight,
    z_weight,
    bc_weight,
    dt_weight,
    x_kernel,
    bc_kernel,
    dt_bias,
    decay_log,
    skip_scale,
    output_gain,
    output_weight,
    saved_states,
    x_history,
    bc_history,
    accepted,
):
    shape = jax.ShapeDtypeStruct
    lines = KV_SIZE * LINES
    x_rows = jnp.transpose(x_history, (1, 0, 2))
    bc_rows = jnp.transpose(bc_history, (1, 0, 2))
    with jax.named_scope("project"):
        near = pl.pallas_call(
            project_body,
            out_shape=shape((TP * NEAR_KV, 2 * TOKENS, 128), BF16),
            in_specs=[smem()] + [vmem()] * 8,
            out_specs=vmem(),
            scratch_shapes=[pltpu.VMEM((128, 128), F32), pltpu.VMEM((128, 128), F32)],
        )(accepted, hidden, input_gain, x_weight.T, z_weight.T, bc_weight.T, dt_weight.T, bc_rows, bc_kernel)
    with jax.named_scope("near"):
        arrived = lax.all_to_all(near, NEAR, 0, 0, tiled=True)
    with jax.named_scope("prepare"):
        first_state, turned_weight = pl.pallas_call(
            prepare_body,
            out_shape=(shape((SEQS, HEAD, STATE), F32), shape((lines, 256), BF16)),
            in_specs=[smem(), pl.BlockSpec(memory_space=pl.ANY), vmem()],
            out_specs=(vmem(), vmem()),
            scratch_shapes=[pltpu.SemaphoreType.DMA((SEQS,))],
            cost_estimate=pl.CostEstimate(flops=4_000_000, bytes_accessed=3_000_000, transcendentals=0),
        )(accepted, saved_states, output_weight)
        gain_row = output_gain.reshape(1, HEAD)
    with jax.named_scope("mix"):
        far, x_window, bc_window, inputs, b_terms, decay = pl.pallas_call(
            mix_body,
            out_shape=(
                shape((lines, 128), BF16),
                shape((7, SEQS, HEAD), BF16),
                shape((7, SEQS, HEAD), BF16),
                shape((TOKENS, 128), F32),
                shape((TOKENS, 128), F32),
                shape((TOKENS, 128), F32),
            ),
            in_specs=[smem()] * 4 + [vmem()] * 6,
            out_specs=(vmem(),) * 6,
            scratch_shapes=[
                pltpu.VMEM((TOKENS, 8), F32),
                pltpu.VMEM((TOKENS, 128), F32),
                pltpu.VMEM((TOKENS, 128), F32),
            ],
        )(
            accepted,
            dt_bias,
            decay_log,
            skip_scale,
            arrived,
            first_state,
            turned_weight,
            x_kernel,
            x_rows,
            gain_row,
        )
    with jax.named_scope("far"):
        landed = lax.all_to_all(far.reshape(KV_SIZE, LINES // 2, 2, 128), KV, 0, 0, tiled=True)
    with jax.named_scope("states"):
        new_states = pl.pallas_call(
            state_body,
            out_shape=shape((SEQS, PROPS + 1, 1, HEAD, STATE), F32),
            in_specs=[vmem()] * 4,
            out_specs=vmem(),
            cost_estimate=pl.CostEstimate(flops=4_000_000, bytes_accessed=3_000_000, transcendentals=0),
        )(inputs, b_terms, decay, first_state)
    with jax.named_scope("finish"):
        mixed = pl.pallas_call(
            finish_body,
            out_shape=shape((TOKENS, TOKENS), BF16),
            in_specs=[vmem()],
            out_specs=vmem(),
            scratch_shapes=[pltpu.VMEM((8 * LINES, 128), F32)],
        )(landed.reshape(lines, 128))
    return (mixed, new_states, jnp.transpose(x_window, (1, 0, 2)), jnp.transpose(bc_window, (1, 0, 2)))


def solution(mesh):
    split = Mesh(mesh.devices.reshape(8, 4, 2, 2, mesh.shape["tp"]), ("z", "yh", "yl", "c", "tp"))
    return jax.shard_map(
        local,
        mesh=split,
        in_specs=(
            P(None, "tp"),
            P("tp"),
            P("tp", KV),
            P("tp", KV),
            P("tp", KV),
            P("tp", KV),
            P(None, KV),
            P(None, KV),
            P(KV),
            P(KV),
            P(KV),
            P(KV),
            P(KV, None),
            P("tp", None, KV, None, None),
            P("tp", None, KV),
            P("tp", None, KV),
            P("tp"),
        ),
        out_specs=(
            P("tp", KV),
            P("tp", None, KV, None, None),
            P("tp", None, KV),
            P("tp", None, KV),
        ),
        check_vma=False,
    )
```

```python
import jax
import jax.numpy as jnp
from jax import lax
from jax.experimental import pallas as pl
from jax.experimental.pallas import tpu as pltpu
from jax.sharding import Mesh
from jax.sharding import PartitionSpec as P

D = 4096
PROPS = 4
INNER = 8192
KV = ("z", "yh", "yl", "c")
NEAR = ("yl", "c", "tp")
EPSILON = 1e-05
TP = 4
NEAR_KV = 4
KV_SIZE = 128
SEQS = 8
TOKENS = 32
HEAD = 64
STATE = 128
LINES = 10

F32 = jnp.float32
BF16 = jnp.bfloat16


def rounded(value):
    return value.astype(BF16).astype(F32)


def lanes_of(shape):
    return lax.broadcasted_iota(jnp.int32, shape, len(shape) - 1)


def rows_of(shape):
    return lax.broadcasted_iota(jnp.int32, shape, len(shape) - 2)


def dot_nt(a, b):
    return lax.dot_general(a, b, (((1,), (1,)), ((), ())), preferred_element_type=F32)


def silu(v):
    return v / (1.0 + jnp.exp(-v))


def accepted_column(accepted):
    line = jnp.broadcast_to(accepted[...].astype(F32)[None, :], (SEQS, SEQS))
    own = lanes_of((SEQS, SEQS)) == rows_of((SEQS, SEQS))
    return jnp.sum(jnp.where(own, line, 0.0), axis=1, keepdims=True)


def kept_rows(history, column):
    whole = [history[i].astype(F32) for i in range(7)]
    kept = []
    for m in range(3):
        row = whole[m]
        for a in range(1, PROPS + 1):
            row = jnp.where(column == float(a), whole[m + a], row)
        kept.append(row)
    return kept


def project_body(
    accepted, hidden, gain, x_weight, z_weight, bc_weight, dt_weight, bc_history, bc_kernel, message, first, second
):
    widened = hidden[...].astype(F32)
    scaled = (widened * gain[...].astype(F32)[None, :]).astype(BF16)
    squares = jnp.sum(widened * widened, axis=1, keepdims=True)
    dt_rows = jnp.broadcast_to(dt_weight[...], (HEAD, dt_weight.shape[1]))
    first[...] = dot_nt(scaled, jnp.concatenate([x_weight[...], z_weight[...]], axis=0))
    last = dot_nt(scaled, jnp.concatenate([bc_weight[...], dt_rows], axis=0))
    second[...] = last
    turned = jnp.transpose(jnp.where(lanes_of((128, 128)) == HEAD + 1, squares, last))
    dt_line = jnp.broadcast_to(turned[HEAD : HEAD + 1], (8, 128))
    square_line = jnp.broadcast_to(turned[HEAD + 1 : HEAD + 2], (8, 128))
    square_high = rounded(square_line)
    rows = rows_of((8, 128))
    upper = lanes_of((8, 128)) >= HEAD
    lines = jnp.where(rows == 4, dt_line, jnp.where(rows == 5, square_high, square_line - square_high))
    column = accepted_column(accepted)
    empty = jnp.zeros((SEQS, HEAD), F32)
    extra = [jnp.concatenate([empty, row], axis=1) for row in kept_rows(bc_history, column)]
    taps = jnp.concatenate([bc_kernel[...].astype(F32), jnp.zeros((4, HEAD), F32)], axis=0)
    taps = jnp.concatenate([empty, taps], axis=1)
    for j in range(TP):
        top = [first[pl.ds(TOKENS * j + t, SEQS, stride=PROPS), :] for t in range(PROPS)]
        low = [second[pl.ds(TOKENS * j + t, SEQS, stride=PROPS), :] for t in range(PROPS)]
        ending = jnp.where(rows < 4, taps, pltpu.roll(lines, (64 - 32 * j) % 128, 1))
        low = [jnp.where(upper, e, v) for e, v in zip([*extra, ending], low)]
        block = jnp.concatenate(top + low, axis=0).astype(BF16)
        for g in range(NEAR_KV):
            message[g * TP + j] = block


def prepare_body(accepted, saved, first_state, arrivals):
    copies = [
        pltpu.make_async_copy(saved.at[s, accepted[s], 0], first_state.at[s], arrivals.at[s]) for s in range(SEQS)
    ]
    for copy in copies:
        copy.start()
    for copy in copies:
        copy.wait()


def mix_body(
    accepted,
    dt_bias,
    decay_log,
    skip_scale,
    arrived,
    first_state,
    weight,
    x_kernel,
    x_history,
    output_gain,
    message,
    x_window,
    bc_window,
    inputs_out,
    b_out,
    decay_out,
    columns,
):
    place = lax.axis_index(("yl", "c"))
    mine = lax.axis_index("tp")
    tile = (SEQS, 128)
    lanes = lanes_of(tile)
    rows = rows_of(tile)
    lower = lanes < HEAD

    def tiles(value):
        return [value[8 * i : 8 * i + 8] for i in range(value.shape[0] // 8)]

    own = arrived[place * TP].astype(F32)
    for k in range(1, TP):
        own = own + arrived[place * TP + k].astype(F32)
    own = tiles(own)
    ending = own[7]
    mean = (ending[5:6] + ending[6:7]) / D
    lined = jnp.where(rows == 5, jnp.broadcast_to(lax.rsqrt(mean + EPSILON), tile), ending)
    columns[...] = jnp.transpose(lined)[HEAD : HEAD + TOKENS]
    scale, step, cumulated = [], [], []
    bias = dt_bias[...].reshape(1, 1)
    skip = skip_scale[...].reshape(1, 1)
    rate = jnp.exp(decay_log[...].reshape(1, 1))
    total = jnp.zeros((SEQS, 1), F32)
    for t in range(PROPS):
        column = columns[pl.ds(t, SEQS, stride=PROPS), :]
        scale.append(column[:, 5:6])
        raw = rounded(column[:, 5:6] * column[:, 4:5]) + bias
        step.append(jnp.maximum(raw, 0.0) + jnp.log1p(jnp.exp(-jnp.abs(raw))))
        total = total - rate * step[t]
        cumulated.append(total)
    fresh = [rounded(scale[t] * own[t]) for t in range(PROPS)]
    sums, extras = [], []
    for g in range(NEAR_KV):
        group = arrived[g * TP, 32:64, :].astype(F32)
        for k in range(1, TP):
            group = group + arrived[g * TP + k, 32:64, :].astype(F32)
        sums.append(tiles(group))
        extras.append(tiles(arrived[g * TP + mine, 32:64, :].astype(F32)))

    def convolved(window, taps):
        results = []
        for t in range(PROPS):
            running = window[t] * taps[0:1]
            for j in range(1, 4):
                running = running + window[t + j] * taps[j : j + 1]
            results.append(silu(running))
        return results

    def terms(left, right):
        window = [
            jnp.where(lower, pltpu.roll(extras[left][m], HEAD, 1), extras[right][m]) for m in range(4)
        ]
        new = [
            rounded(scale[t] * jnp.where(lower, sums[left][t], pltpu.roll(sums[right][t], HEAD, 1)))
            for t in range(PROPS)
        ]
        return convolved(window[:3] + new, window[3])

    b_terms = terms(0, 1)
    c_terms = terms(2, 3)
    column = accepted_column(accepted)
    kept = kept_rows(x_history, column)
    empty = jnp.zeros((SEQS, HEAD), F32)
    x_taps = jnp.concatenate([x_kernel[...].astype(F32), jnp.zeros((4, HEAD), F32)], axis=1)
    x_conv = convolved([jnp.concatenate([row, empty], axis=1) for row in kept] + fresh, x_taps)
    states = first_state[...].reshape(SEQS * HEAD, STATE).astype(BF16)
    read = dot_nt(jnp.concatenate(c_terms, axis=0).astype(BF16), states)
    gain = output_gain[...].astype(F32)
    gain = jnp.concatenate([gain, gain], axis=1)
    scaled = []
    squares = jnp.zeros(tile, F32)
    for t in range(PROPS):
        picked = jnp.zeros(tile, F32)
        for k in range(SEQS // 2):
            picked = jnp.where(rows // 2 == k, read[8 * t : 8 * t + 8, 128 * k : 128 * k + 128], picked)
        picked = jnp.where(rows % 2 == 0, picked, pltpu.roll(picked, HEAD, 1))
        output = jnp.exp(cumulated[t]) * picked
        for r in range(t + 1):
            product = jnp.sum(c_terms[t] * b_terms[r], axis=1, keepdims=True)
            output = output + (jnp.exp(cumulated[t] - cumulated[r]) * step[r] * product) * x_conv[r]
        output = output + skip * x_conv[t]
        gated = jnp.where(lower, output * silu(pltpu.roll(fresh[t], HEAD, 1)), 0.0)
        square = jnp.sum(gated * gated, axis=1, keepdims=True)
        scaled.append(jnp.where(lower, gated * gain, 0.0)[:, :HEAD])
        squares = jnp.where(lanes // TOKENS == t, square, squares)
        inputs_out[8 * t : 8 * t + 8, :] = x_conv[t] * step[t]
        b_out[8 * t : 8 * t + 8, :] = b_terms[t]
        decay_out[8 * t : 8 * t + 8, :] = jnp.broadcast_to(jnp.exp(-rate * step[t]), tile)
    turns = []
    for d in range(4):
        turns += [row if d == 0 else pltpu.roll(row, 2 * d, 0) for row in scaled]
    turns = jnp.concatenate(turns, axis=0).astype(BF16)
    square_line = jnp.sum(jnp.where(lanes % TOKENS == rows, squares, 0.0), axis=0, keepdims=True)
    high = rounded(square_line)
    lines = jnp.where(rows % 2 == 0, high, square_line - high)
    quarter = lanes // TOKENS
    for i in range(weight.shape[1] // 256):
        product = jnp.dot(turns, weight[:, 256 * i : 256 * (i + 1)], preferred_element_type=F32)
        pieces = []
        for half in range(2):
            block = product[:, 128 * half : 128 * (half + 1)]
            spots = []
            for d in range(4):
                spot = None
                for q in range(4):
                    piece = block[32 * d + 8 * q : 32 * d + 8 * q + 8]
                    piece = piece if q == d else pltpu.roll(piece, (32 * (q - d)) % 128, 1)
                    spot = piece if q == 0 else jnp.where(quarter == q, piece, spot)
                spots.append(spot)
            pieces += [
                spots[0],
                jnp.where(rows < 2, lines, spots[1]),
                jnp.where(rows < 2, spots[1], jnp.where(rows < 4, lines, spots[2])),
                jnp.where(rows < 4, spots[2], jnp.where(rows < 6, lines, spots[3])),
                jnp.where(rows < 6, spots[3], lines),
            ]
        message[80 * i : 80 * (i + 1), :] = jnp.concatenate(pieces, axis=0).astype(BF16)
    own_extra = tiles(arrived[place * TP + mine, 32:64, :].astype(F32))
    for m in range(3):
        x_window[m] = kept[m].astype(BF16)
        bc_window[m] = pltpu.roll(own_extra[m], HEAD, 1)[:, :HEAD].astype(BF16)
    for t in range(PROPS):
        x_window[3 + t] = fresh[t][:, :HEAD].astype(BF16)
        bc_window[3 + t] = (scale[t] * own[4 + t])[:, :HEAD].astype(BF16)


def state_body(inputs, b_terms, decay, first_state, new_states):
    padded = jnp.concatenate([inputs[...], jnp.zeros((128 - TOKENS, 128), F32)], axis=0)
    turned = jnp.transpose(padded)[:HEAD]
    for s in range(SEQS):
        state = first_state[s]
        new_states[s, 0, 0] = state
        for t in range(PROPS):
            at = 8 * t + s
            state = state * decay[at : at + 1, :] + turned[:, at : at + 1] * b_terms[at : at + 1, :]
            new_states[s, t + 1, 0] = state


def finish_body(arrived, mixed, total, placed):
    step = 8 * LINES
    running = arrived[0:step, :].astype(F32)
    for i in range(1, arrived.shape[0] // step):
        running = running + arrived[step * i : step * (i + 1), :].astype(F32)
    total[...] = running
    summed = total[0:8, :]
    squares = total[8:10, :]
    for i in range(1, 8):
        summed = summed + total[LINES * i : LINES * i + 8, :]
        squares = squares + total[LINES * i + 8 : LINES * i + 10, :]
    mean = jnp.broadcast_to((squares[0:1] + squares[1:2]) / INNER, (8, 128))
    lanes = lanes_of((8, 128))
    rows = rows_of((8, 128))
    for t in range(PROPS):
        own = jnp.sum(jnp.where(lanes == TOKENS * t + rows, mean, 0.0), axis=1, keepdims=True)
        moved = summed if t == 0 else pltpu.roll(summed, 128 - TOKENS * t, 1)
        placed[pl.ds(t, SEQS, stride=PROPS), :] = lax.rsqrt(own + EPSILON) * moved
    mixed[...] = placed[...][:, :TOKENS].astype(BF16)


def smem():
    return pl.BlockSpec(memory_space=pltpu.SMEM)


def vmem():
    return pl.BlockSpec(memory_space=pltpu.VMEM)


def near_memory(value):
    return pltpu.with_memory_space_constraint(value, pltpu.VMEM)


def local(
    hidden,
    input_gain,
    x_weight,
    z_weight,
    bc_weight,
    dt_weight,
    x_kernel,
    bc_kernel,
    dt_bias,
    decay_log,
    skip_scale,
    output_gain,
    output_weight,
    saved_states,
    x_history,
    bc_history,
    accepted,
):
    shape = jax.ShapeDtypeStruct
    held = pltpu.VMEM
    lines = KV_SIZE * LINES
    x_rows = jnp.transpose(x_history, (1, 0, 2))
    bc_rows = jnp.transpose(bc_history, (1, 0, 2))
    with jax.named_scope("project"):
        near = pl.pallas_call(
            project_body,
            out_shape=held((TP * NEAR_KV, 2 * TOKENS, 128), BF16),
            in_specs=[vmem()] * 9,
            out_specs=vmem(),
            scratch_shapes=[pltpu.VMEM((128, 128), F32), pltpu.VMEM((128, 128), F32)],
        )(accepted, hidden, input_gain, x_weight.T, z_weight.T, bc_weight.T, dt_weight.T, bc_rows, bc_kernel)
    with jax.named_scope("near"):
        arrived = near_memory(lax.all_to_all(near, NEAR, 0, 0, tiled=True))
    with jax.named_scope("prepare"):
        first_state = pl.pallas_call(
            prepare_body,
            out_shape=held((SEQS, HEAD, STATE), F32),
            in_specs=[smem(), pl.BlockSpec(memory_space=pl.ANY)],
            out_specs=vmem(),
            scratch_shapes=[pltpu.SemaphoreType.DMA((SEQS,))],
            cost_estimate=pl.CostEstimate(flops=4_000_000, bytes_accessed=3_000_000, transcendentals=0),
        )(accepted, saved_states)
        first_state = near_memory(first_state)
    with jax.named_scope("mix"):
        far, x_window, bc_window, inputs, b_terms, decay = pl.pallas_call(
            mix_body,
            out_shape=(
                held((lines, 128), BF16),
                shape((7, SEQS, HEAD), BF16),
                shape((7, SEQS, HEAD), BF16),
                held((TOKENS, 128), F32),
                held((TOKENS, 128), F32),
                held((TOKENS, 128), F32),
            ),
            in_specs=[vmem()] * 10,
            out_specs=(vmem(),) * 6,
            scratch_shapes=[pltpu.VMEM((TOKENS, 8), F32)],
        )(
            accepted,
            dt_bias,
            decay_log,
            skip_scale,
            arrived,
            first_state,
            near_memory(output_weight),
            x_kernel,
            x_rows,
            output_gain.reshape(1, HEAD),
        )
    with jax.named_scope("far"):
        landed = lax.all_to_all(far.reshape(KV_SIZE, LINES // 2, 2, 128), KV, 0, 0, tiled=True)
        landed = near_memory(landed.reshape(lines, 128))
    with jax.named_scope("states"):
        new_states = pl.pallas_call(
            state_body,
            out_shape=shape((SEQS, PROPS + 1, 1, HEAD, STATE), F32),
            in_specs=[vmem()] * 4,
            out_specs=vmem(),
            cost_estimate=pl.CostEstimate(flops=4_000_000, bytes_accessed=3_000_000, transcendentals=0),
        )(near_memory(inputs), near_memory(b_terms), near_memory(decay), first_state)
    with jax.named_scope("finish"):
        mixed = pl.pallas_call(
            finish_body,
            out_shape=shape((TOKENS, TOKENS), BF16),
            in_specs=[vmem()],
            out_specs=vmem(),
            scratch_shapes=[pltpu.VMEM((8 * LINES, 128), F32), pltpu.VMEM((TOKENS, 128), F32)],
        )(landed)
    return (mixed, new_states, jnp.transpose(x_window, (1, 0, 2)), jnp.transpose(bc_window, (1, 0, 2)))


def solution(mesh):
    split = Mesh(mesh.devices.reshape(8, 4, 2, 2, mesh.shape["tp"]), ("z", "yh", "yl", "c", "tp"))
    return jax.shard_map(
        local,
        mesh=split,
        in_specs=(
            P(None, "tp"),
            P("tp"),
            P("tp", KV),
            P("tp", KV),
            P("tp", KV),
            P("tp", KV),
            P(None, KV),
            P(None, KV),
            P(KV),
            P(KV),
            P(KV),
            P(KV),
            P(KV, None),
            P("tp", None, KV, None, None),
            P("tp", None, KV),
            P("tp", None, KV),
            P("tp"),
        ),
        out_specs=(
            P("tp", KV),
            P("tp", None, KV, None, None),
            P("tp", None, KV),
            P("tp", None, KV),
        ),
        check_vma=False,
    )
```

```python
import jax
import jax.numpy as jnp
from jax import lax
from jax.experimental import pallas as pl
from jax.experimental.pallas import tpu as pltpu
from jax.sharding import Mesh
from jax.sharding import PartitionSpec as P


D = 4096
PROPS = 4
INNER = 8192
KV = ("z", "yh", "yl", "c")
NEAR = ("yl", "c", "tp")
EPSILON = 1e-05
TP = 4
NEAR_KV = 4
KV_SIZE = 128
SEQS = 8
HALF = 4
TOKENS = 32
HEAD = 64
STATE = 128
LINES = 6
TILE = (8, 128)
SMALL = 64

F32 = jnp.float32
BF16 = jnp.bfloat16


def rounded(value):
    return value.astype(BF16).astype(F32)


def lanes_of(shape):
    return lax.broadcasted_iota(jnp.int32, shape, len(shape) - 1)


def rows_of(shape):
    return lax.broadcasted_iota(jnp.int32, shape, len(shape) - 2)


def dot_nt(a, b):
    return lax.dot_general(a, b, (((1,), (1,)), ((), ())), preferred_element_type=F32)


def silu(v):
    return v / (1.0 + jnp.exp(-v))


def softplus(v):
    return jnp.maximum(v, 0.0) + jnp.log1p(jnp.exp(-jnp.abs(v)))


def tiles(value):
    return [value[8 * i : 8 * i + 8] for i in range(value.shape[0] // 8)]


def swapped(tile):
    return pltpu.roll(tile, HEAD, 1)


def turned_half(tile):
    return pltpu.roll(tile, HALF, 0)


def widened(tile):
    return jnp.concatenate([tile, jnp.zeros(tile.shape, tile.dtype)], axis=1)


def kept_rows(history, accepted):
    rows = rows_of((SEQS, HEAD))
    column = jnp.zeros((SEQS, HEAD), jnp.int32)
    for s in range(SEQS):
        column = jnp.where(rows == s, accepted[s], column)
    whole = [history[i].astype(F32) for i in range(7)]
    kept = []
    for m in range(3):
        row = whole[m]
        for a in range(1, PROPS + 1):
            row = jnp.where(column == a, whole[m + a], row)
        kept.append(row)
    return kept


def convolved(window, taps):
    results = []
    for t in range(PROPS):
        running = window[t] * taps[0]
        for j in range(1, 4):
            running = running + window[t + j] * taps[j]
        results.append(silu(running))
    return results


def three_terms(value, shape):
    value = jnp.broadcast_to(value, shape)
    high = rounded(value)
    middle = rounded(value - high)
    lanes = lanes_of(shape)
    low = value - high - middle
    return jnp.where(lanes == HEAD, high, jnp.where(lanes == HEAD + 1, middle, jnp.where(lanes == HEAD + 2, low, 0.0)))


def project_body(
    accepted,
    saved,
    hidden,
    gain,
    x_weight,
    z_weight,
    bc_weight,
    dt_weight,
    bc_history,
    bc_kernel,
    message,
    first_state,
    first,
    second,
    arrivals,
):
    copies = [
        pltpu.make_async_copy(saved.at[s, accepted[s], 0], first_state.at[s], arrivals.at[s]) for s in range(SEQS)
    ]
    for copy in copies:
        copy.start()
    wide = hidden[...].astype(F32)
    scaled = (wide * gain[...].astype(F32)[None, :]).astype(BF16)
    squares = jnp.sum(wide * wide, axis=1, keepdims=True)
    dt_rows = jnp.broadcast_to(dt_weight[...], (HEAD, dt_weight.shape[1]))
    first[...] = dot_nt(scaled, jnp.concatenate([x_weight[...], z_weight[...]], axis=0))
    last = dot_nt(scaled, jnp.concatenate([bc_weight[...], dt_rows], axis=0))
    second[...] = last
    turned = jnp.transpose(jnp.where(lanes_of((128, 128)) == HEAD + 1, squares, last))
    dt_line = jnp.broadcast_to(turned[HEAD : HEAD + 1], TILE)
    square_line = jnp.broadcast_to(turned[HEAD + 1 : HEAD + 2], TILE)
    square_high = rounded(square_line)
    rows = rows_of(TILE)
    upper = lanes_of(TILE) >= HEAD
    lines = jnp.where(rows == 4, dt_line, jnp.where(rows == 5, square_high, square_line - square_high))
    empty = jnp.zeros((SEQS, HEAD), F32)
    extra = [jnp.concatenate([empty, row], axis=1) for row in kept_rows(bc_history, accepted)]
    taps = jnp.concatenate([bc_kernel[...].astype(F32), jnp.zeros((4, HEAD), F32)], axis=0)
    taps = jnp.concatenate([empty, taps], axis=1)
    for j in range(TP):
        top = [first[pl.ds(TOKENS * j + t, SEQS, stride=PROPS), :] for t in range(PROPS)]
        low = [second[pl.ds(TOKENS * j + t, SEQS, stride=PROPS), :] for t in range(PROPS)]
        ending = jnp.where(rows < 4, taps, pltpu.roll(lines, (64 - 32 * j) % 128, 1))
        low = [jnp.where(upper, e, v) for e, v in zip([*extra, ending], low)]
        block = jnp.concatenate(top + low, axis=0).astype(BF16)
        for g in range(NEAR_KV):
            message[g * TP + j] = block
    for copy in copies:
        copy.wait()


def pack_body(
    accepted,
    dt_bias,
    decay_log,
    skip_scale,
    first_state,
    weight,
    x_history,
    x_kernel,
    output_gain,
    kept_pack,
    sent,
):
    core = lax.axis_index("c")
    rows = rows_of(TILE)
    terms = [three_terms(number[0], TILE) for number in (dt_bias, decay_log, skip_scale)]
    gain_row = jnp.concatenate([jnp.zeros((1, HEAD), F32), output_gain[...].astype(F32)], axis=1)
    kernel = x_kernel[...].astype(F32)
    small = [widened(row) for row in kept_rows(x_history, accepted)]
    small = [jnp.where(core == 1, turned_half(tile), tile) for tile in small]
    small += [jnp.broadcast_to(widened(kernel[j : j + 1]), TILE) for j in range(4)]
    small = [small[0] + gain_row] + [a + b for a, b in zip(small[1:4], terms)] + small[4:]
    small.append(jnp.zeros(TILE, F32))
    kept_pack[0:SMALL, :] = jnp.concatenate([jnp.where(rows < HALF, tile, 0.0) for tile in small], axis=0).astype(BF16)
    kept_pack[SMALL:, :] = first_state[pl.ds(HALF * core, HALF)].reshape(HALF * HEAD, STATE).astype(BF16)
    sent[0:HEAD, :] = weight[...]
    small = [jnp.where(rows < HALF, 0.0, tile) for tile in small]
    states = first_state[pl.ds(HALF - HALF * core, HALF)].reshape(HALF * HEAD, STATE)
    blocks = [jnp.concatenate(small[2 * i : 2 * i + 2], axis=0) for i in range(SMALL // 16)]
    blocks += [states[16 * i : 16 * i + 16] for i in range(HALF * HEAD // 16)]
    blocks += [jnp.zeros((16, 128), F32)] * (weight.shape[1] // 128 - len(blocks))
    for i, block in enumerate(blocks):
        sent[HEAD : HEAD + 16, 128 * i : 128 * i + 128] = block.astype(BF16)


def summed_over_tp(arrived, place, start):
    total = arrived[place * TP, start : 2 * TOKENS, :].astype(F32)
    for k in range(1, TP):
        total = total + arrived[place * TP + k, start : 2 * TOKENS, :].astype(F32)
    return tiles(total)


def scale_line(ending):
    return lax.rsqrt((ending[5:6] + ending[6:7]) / D + EPSILON)


def mix_body(arrived, kept_pack, got, weight, message, columns):
    core = lax.axis_index("c")
    pair = lax.axis_index("yl") * 2
    mine = lax.axis_index("tp")
    lanes = lanes_of(TILE)
    rows = rows_of(TILE)
    lower = lanes < HEAD
    first_rows = rows < HALF
    second_core = core == 1

    def halves(own, other):
        own = jnp.where(second_core, turned_half(own), own)
        other = jnp.where(second_core, other, turned_half(other))
        return jnp.where(rows_of(own.shape) < HALF, own, other)

    own = summed_over_tp(arrived, pair + core, 0)
    other = summed_over_tp(arrived, pair + 1 - core, 0)
    got_small = [got[HEAD : HEAD + 16, 128 * i : 128 * i + 128] for i in range(SMALL // 16)]
    small = tiles(kept_pack[0:SMALL, :].astype(F32) + jnp.concatenate(got_small, axis=0).astype(F32))
    gain = swapped(small[0])
    bias, decay, skip = [
        tile[:, HEAD : HEAD + 1] + tile[:, HEAD + 1 : HEAD + 2] + tile[:, HEAD + 2 : HEAD + 3] for tile in small[1:4]
    ]
    ending = own[7]
    lined = jnp.where(rows == 0, jnp.broadcast_to(scale_line(ending), TILE), ending)
    lined = jnp.where(rows == 1, jnp.broadcast_to(other[7][4:5], TILE), lined)
    columns[...] = jnp.transpose(lined)[HEAD : HEAD + TOKENS]
    rate = jnp.exp(decay)
    scale, step, cumulated = [], [], []
    total = jnp.zeros((SEQS, 1), F32)
    for t in range(PROPS):
        column = columns[pl.ds(t, SEQS, stride=PROPS), :]
        column = halves(column, column)
        scale.append(column[:, 0:1])
        raw = jnp.where(rows_of((SEQS, 1)) < HALF, column[:, 4:5], column[:, 1:2])
        step.append(softplus(rounded(scale[t] * raw) + bias))
        total = total - rate * step[t]
        cumulated.append(total)
    fresh = [rounded(scale[t] * halves(own[t], other[t])) for t in range(PROPS)]
    sums, extras = [], []
    for g in range(NEAR_KV):
        sums.append(summed_over_tp(arrived, g, TOKENS))
        extras.append(tiles(arrived[g * TP + mine, TOKENS : 2 * TOKENS, :].astype(F32)))

    def terms(left, right):
        window = [jnp.where(lower, swapped(extras[left][m]), extras[right][m]) for m in range(4)]
        new = [jnp.where(lower, sums[left][t], swapped(sums[right][t])) for t in range(PROPS)]
        taps = [window[3][j : j + 1] for j in range(4)]
        window = [halves(tile, tile) for tile in window[:3]]
        return convolved(window + [rounded(scale[t] * halves(new[t], new[t])) for t in range(PROPS)], taps)

    b_terms = terms(0, 1)
    c_terms = terms(2, 3)
    x_conv = convolved(small[0:3] + fresh, small[3:7])
    spans = range(SMALL // 16, (SMALL + HALF * HEAD) // 16)
    got_states = [got[HEAD : HEAD + 16, 128 * i : 128 * i + 128] for i in spans]
    states = jnp.concatenate([kept_pack[SMALL:, :], *got_states], axis=0)
    read = dot_nt(jnp.concatenate(c_terms, axis=0).astype(BF16), states)
    scaled = []
    squares = jnp.zeros(TILE, F32)
    quarter = lanes // TOKENS
    for t in range(PROPS):
        picked = jnp.zeros(TILE, F32)
        for k in range(SEQS // 2):
            picked = jnp.where(rows // 2 == k, read[8 * t : 8 * t + 8, 128 * k : 128 * k + 128], picked)
        picked = jnp.where(rows % 2 == 0, picked, swapped(picked))
        output = jnp.exp(cumulated[t]) * picked
        for r in range(t + 1):
            product = jnp.sum(c_terms[t] * b_terms[r], axis=1, keepdims=True)
            output = output + (jnp.exp(cumulated[t] - cumulated[r]) * step[r] * product) * x_conv[r]
        output = output + skip * x_conv[t]
        gated = output * silu(swapped(fresh[t]))
        both = jnp.where(lower, gated, swapped(turned_half(gated)))
        squares = jnp.where(quarter == t, jnp.sum(both * both, axis=1, keepdims=True), squares)
        gains = jnp.where(lower, gain, swapped(turned_half(gain)))
        scaled.append(both * gains)
    turns = []
    for d in range(4):
        turns += [row if d == 0 else pltpu.roll(row, 8 - 2 * d, 0) for row in scaled]
    turns = jnp.concatenate(turns, axis=0).astype(BF16)
    spot = jnp.where(first_rows & (lanes % TOKENS == rows), squares, 0.0)
    square_line = jnp.sum(spot, axis=0, keepdims=True)
    high = rounded(square_line)
    lines = jnp.where(rows % 2 == 0, high, square_line - high)
    for i in range(weight.shape[1] // 256):
        cut = slice(256 * i, 256 * (i + 1))
        both_weights = jnp.concatenate([weight[:, cut], got[0:HEAD, cut]], axis=0)
        product = jnp.dot(turns, both_weights, preferred_element_type=F32)
        pieces = []
        for half in range(2):
            block = product[:, 128 * half : 128 * (half + 1)]
            spots = []
            for d in range(4):
                spot = None
                for t in range(PROPS):
                    piece = block[32 * d + 8 * t : 32 * d + 8 * t + 8]
                    piece = piece if t == d else pltpu.roll(piece, (32 * (t - d)) % 128, 1)
                    spot = piece if t == 0 else jnp.where(quarter == t, piece, spot)
                spots.append(spot)
            pieces += [
                jnp.where(rows < 4, spots[0], jnp.where(rows < 6, lines, spots[1])),
                jnp.where(rows < 2, spots[1], jnp.where(rows < 4, lines, spots[2])),
                jnp.where((rows >= 2) & (rows < 6), spots[3], lines),
            ]
        message[48 * i : 48 * (i + 1), :] = jnp.concatenate(pieces, axis=0).astype(BF16)


def state_body(
    accepted,
    dt_bias,
    decay_log,
    arrived,
    first_state,
    x_kernel,
    x_history,
    new_states,
    x_window,
    bc_window,
    columns,
):
    place = lax.axis_index(("yl", "c"))
    mine = lax.axis_index("tp")
    lanes = lanes_of(TILE)
    lower = lanes < HEAD
    own = summed_over_tp(arrived, place, 0)
    ending = own[7]
    lined = jnp.where(rows_of(TILE) == 0, jnp.broadcast_to(scale_line(ending), TILE), ending)
    columns[...] = jnp.transpose(lined)[HEAD : HEAD + TOKENS]
    bias = dt_bias[0]
    rate = jnp.exp(jnp.full((SEQS, 1), decay_log[0], F32))
    scale, step = [], []
    for t in range(PROPS):
        column = columns[pl.ds(t, SEQS, stride=PROPS), :]
        scale.append(column[:, 0:1])
        step.append(softplus(rounded(scale[t] * column[:, 4:5]) + bias))
    fresh = [rounded(scale[t] * own[t]) for t in range(PROPS)]
    sums = [summed_over_tp(arrived, g, TOKENS) for g in range(2)]
    extras = [tiles(arrived[g * TP + mine, TOKENS : 2 * TOKENS, :].astype(F32)) for g in range(2)]
    window = [jnp.where(lower, swapped(extras[0][m]), extras[1][m]) for m in range(4)]
    new = [rounded(scale[t] * jnp.where(lower, sums[0][t], swapped(sums[1][t]))) for t in range(PROPS)]
    b_terms = convolved(window[:3] + new, [window[3][j : j + 1] for j in range(4)])
    kept = kept_rows(x_history, accepted)
    kernel = widened(x_kernel[...].astype(F32))
    x_conv = convolved([widened(row) for row in kept] + fresh, [kernel[j : j + 1] for j in range(4)])
    inputs = [x_conv[t] * step[t] for t in range(PROPS)]
    turned = jnp.transpose(jnp.concatenate(inputs + [jnp.zeros((128 - TOKENS, 128), F32)], axis=0))[:HEAD]
    decay = [jnp.broadcast_to(jnp.exp(-rate * step[t]), TILE) for t in range(PROPS)]
    for s in range(SEQS):
        state = first_state[s]
        new_states[s, 0, 0] = state
        for t in range(PROPS):
            at = 8 * t + s
            state = state * decay[t][s : s + 1, :] + turned[:, at : at + 1] * b_terms[t][s : s + 1, :]
            new_states[s, t + 1, 0] = state
    own_extra = tiles(arrived[place * TP + mine, TOKENS : 2 * TOKENS, :].astype(F32))
    for m in range(3):
        x_window[m] = kept[m].astype(BF16)
        bc_window[m] = swapped(own_extra[m])[:, :HEAD].astype(BF16)
    for t in range(PROPS):
        x_window[3 + t] = fresh[t][:, :HEAD].astype(BF16)
        bc_window[3 + t] = (scale[t] * own[4 + t])[:, :HEAD].astype(BF16)


def finish_body(arrived, mixed, total, placed):
    step = 8 * LINES
    running = arrived[0:step, :].astype(F32)
    for i in range(1, arrived.shape[0] // step):
        running = running + arrived[step * i : step * (i + 1), :].astype(F32)
    total[...] = running
    sums = []
    for c in range(2):
        start = LINES * c
        part = total[start : start + LINES, :]
        for i in range(1, 4):
            part = part + total[2 * LINES * i + start : 2 * LINES * i + start + LINES, :]
        sums.append(part)
    summed = jnp.concatenate([part[:HALF] for part in sums], axis=0)
    means = [jnp.broadcast_to((part[4:5] + part[5:6]) / INNER, (HALF, 128)) for part in sums]
    mean = jnp.concatenate(means, axis=0)
    lanes = lanes_of(TILE)
    rows = rows_of(TILE)
    for t in range(PROPS):
        own = jnp.sum(jnp.where(lanes == TOKENS * t + rows % HALF, mean, 0.0), axis=1, keepdims=True)
        moved = summed if t == 0 else pltpu.roll(summed, 128 - TOKENS * t, 1)
        placed[pl.ds(t, SEQS, stride=PROPS), :] = lax.rsqrt(own + EPSILON) * moved
    mixed[...] = placed[...][:, :TOKENS].astype(BF16)


def smem():
    return pl.BlockSpec(memory_space=pltpu.SMEM)


def vmem():
    return pl.BlockSpec(memory_space=pltpu.VMEM)


def far_memory():
    return pl.BlockSpec(memory_space=pltpu.HBM)


def near_memory(value):
    return pltpu.with_memory_space_constraint(value, pltpu.VMEM)


def local(
    hidden,
    input_gain,
    x_weight,
    z_weight,
    bc_weight,
    dt_weight,
    x_kernel,
    bc_kernel,
    dt_bias,
    decay_log,
    skip_scale,
    output_gain,
    output_weight,
    saved_states,
    x_history,
    bc_history,
    accepted,
):
    shape = jax.ShapeDtypeStruct
    held = pltpu.VMEM
    lines = KV_SIZE * LINES
    x_rows = jnp.transpose(x_history, (1, 0, 2))
    bc_rows = jnp.transpose(bc_history, (1, 0, 2))
    pack_rows = SMALL + HALF * HEAD
    near, first_state = pl.pallas_call(
        project_body,
        out_shape=(shape((TP * NEAR_KV, 2 * TOKENS, 128), BF16), held((SEQS, HEAD, STATE), F32)),
        in_specs=[smem(), far_memory()] + [vmem()] * 8,
        out_specs=(vmem(),) * 2,
        scratch_shapes=[pltpu.VMEM((128, 128), F32), pltpu.VMEM((128, 128), F32), pltpu.SemaphoreType.DMA((SEQS,))],
    )(accepted, saved_states, hidden, input_gain, x_weight.T, z_weight.T, bc_weight.T, dt_weight.T, bc_rows, bc_kernel)
    first_state = near_memory(first_state)
    output_weight = near_memory(output_weight)
    arrived = near_memory(lax.all_to_all(near, NEAR, 0, 0, tiled=True))
    kept_pack, sent = pl.pallas_call(
        pack_body,
        out_shape=(held((pack_rows, 128), BF16), held((HEAD + 16, output_weight.shape[1]), BF16)),
        in_specs=[smem()] * 4 + [vmem()] * 5,
        out_specs=(vmem(),) * 2,
        cost_estimate=pl.CostEstimate(flops=4_000_000, bytes_accessed=3_000_000, transcendentals=0),
    )(
        accepted,
        dt_bias,
        decay_log,
        skip_scale,
        first_state,
        output_weight,
        x_rows,
        x_kernel,
        output_gain.reshape(1, HEAD),
    )
    got = lax.ppermute(sent, "c", [(0, 1), (1, 0)])
    far = pl.pallas_call(
        mix_body,
        out_shape=shape((lines, 128), BF16),
        in_specs=[vmem()] * 4,
        out_specs=vmem(),
        scratch_shapes=[pltpu.VMEM((TOKENS, 8), F32)],
    )(arrived, near_memory(kept_pack), near_memory(got), output_weight)
    landed = lax.all_to_all(far.reshape(KV_SIZE, LINES // 2, 2, 128), KV, 0, 0, tiled=True)
    landed = near_memory(landed.reshape(lines, 128))
    new_states, x_window, bc_window = pl.pallas_call(
        state_body,
        out_shape=(
            shape((SEQS, PROPS + 1, 1, HEAD, STATE), F32),
            shape((7, SEQS, HEAD), BF16),
            shape((7, SEQS, HEAD), BF16),
        ),
        in_specs=[smem()] * 3 + [vmem()] * 4,
        out_specs=(vmem(),) * 3,
        scratch_shapes=[pltpu.VMEM((TOKENS, 8), F32)],
        cost_estimate=pl.CostEstimate(flops=4_000_000, bytes_accessed=3_000_000, transcendentals=0),
    )(
        accepted,
        dt_bias,
        decay_log,
        arrived,
        first_state,
        x_kernel,
        x_rows,
    )
    mixed = pl.pallas_call(
        finish_body,
        out_shape=shape((TOKENS, TOKENS), BF16),
        in_specs=[vmem()],
        out_specs=vmem(),
        scratch_shapes=[pltpu.VMEM((8 * LINES, 128), F32), pltpu.VMEM((TOKENS, 128), F32)],
    )(landed)
    return (mixed, new_states, jnp.transpose(x_window, (1, 0, 2)), jnp.transpose(bc_window, (1, 0, 2)))


def solution(mesh):
    split = Mesh(mesh.devices.reshape(8, 4, 2, 2, mesh.shape["tp"]), ("z", "yh", "yl", "c", "tp"))
    return jax.shard_map(
        local,
        mesh=split,
        in_specs=(
            P(None, "tp"),
            P("tp"),
            P("tp", KV),
            P("tp", KV),
            P("tp", KV),
            P("tp", KV),
            P(None, KV),
            P(None, KV),
            P(KV),
            P(KV),
            P(KV),
            P(KV),
            P(KV, None),
            P("tp", None, KV, None, None),
            P("tp", None, KV),
            P("tp", None, KV),
            P("tp"),
        ),
        out_specs=(
            P("tp", KV),
            P("tp", None, KV, None, None),
            P("tp", None, KV),
            P("tp", None, KV),
        ),
        check_vma=False,
    )
```

```python
import jax
import jax.numpy as jnp
from jax import lax
from jax.experimental import pallas as pl
from jax.experimental.pallas import tpu as pltpu
from jax.sharding import Mesh
from jax.sharding import PartitionSpec as P


D = 4096
PROPS = 4
INNER = 8192
KV = ("z", "yh", "yl", "c")
NEAR = ("yl", "c", "tp")
EPSILON = 1e-05
TP = 4
NEAR_KV = 4
KV_SIZE = 128
SEQS = 8
HALF = 4
TOKENS = 32
HEAD = 64
STATE = 128
LINES = 6
TILE = (8, 128)
SMALL = 64

F32 = jnp.float32
BF16 = jnp.bfloat16


def rounded(value):
    return value.astype(BF16).astype(F32)


def lanes_of(shape):
    return lax.broadcasted_iota(jnp.int32, shape, len(shape) - 1)


def rows_of(shape):
    return lax.broadcasted_iota(jnp.int32, shape, len(shape) - 2)


def dot_nt(a, b):
    return lax.dot_general(a, b, (((1,), (1,)), ((), ())), preferred_element_type=F32)


def silu(v):
    return v / (1.0 + jnp.exp(-v))


def softplus(v):
    return jnp.maximum(v, 0.0) + jnp.log1p(jnp.exp(-jnp.abs(v)))


def tiles(value):
    return [value[8 * i : 8 * i + 8] for i in range(value.shape[0] // 8)]


def swapped(tile):
    return pltpu.roll(tile, HEAD, 1)


def turned_half(tile):
    return pltpu.roll(tile, HALF, 0)


def widened(tile):
    return jnp.concatenate([tile, jnp.zeros(tile.shape, tile.dtype)], axis=1)


def kept_rows(history, accepted):
    line = jnp.broadcast_to(accepted[...].astype(F32)[None, :], (SEQS, SEQS))
    own = lanes_of((SEQS, SEQS)) == rows_of((SEQS, SEQS))
    column = jnp.sum(jnp.where(own, line, 0.0), axis=1, keepdims=True)
    whole = [history[i].astype(F32) for i in range(7)]
    kept = []
    for m in range(3):
        row = whole[m]
        for a in range(1, PROPS + 1):
            row = jnp.where(column == float(a), whole[m + a], row)
        kept.append(row)
    return kept


def convolved(window, taps):
    results = []
    for t in range(PROPS):
        running = window[t] * taps[0]
        for j in range(1, 4):
            running = running + window[t + j] * taps[j]
        results.append(silu(running))
    return results


def three_terms(value, shape):
    value = jnp.broadcast_to(value, shape)
    high = rounded(value)
    middle = rounded(value - high)
    lanes = lanes_of(shape)
    low = value - high - middle
    return jnp.where(lanes == HEAD, high, jnp.where(lanes == HEAD + 1, middle, jnp.where(lanes == HEAD + 2, low, 0.0)))


def project_body(
    accepted_far,
    saved,
    hidden_far,
    x_weight_far,
    z_weight_far,
    bc_weight_far,
    gain_far,
    dt_weight_far,
    bc_history_far,
    bc_kernel_far,
    message,
    first_state,
    chosen,
    accepted,
    hidden,
    x_weight,
    z_weight,
    bc_weight,
    gain,
    dt_weight,
    bc_history,
    bc_kernel,
    first,
    second,
    blocks,
    coming,
    reading,
    leaving,
):
    sources = [
        accepted_far,
        hidden_far,
        x_weight_far,
        z_weight_far,
        bc_weight_far,
        gain_far,
        dt_weight_far,
        bc_history_far,
        bc_kernel_far,
        accepted_far,
    ]
    targets = [chosen, hidden, x_weight, z_weight, bc_weight, gain, dt_weight, bc_history, bc_kernel, accepted]
    inputs = [pltpu.make_async_copy(a, b, coming.at[i]) for i, (a, b) in enumerate(zip(sources, targets))]
    for copy in inputs:
        copy.start()
    inputs[0].wait()
    reads = [
        pltpu.make_async_copy(saved.at[s, chosen[s], 0], first_state.at[s], reading.at[s]) for s in range(SEQS)
    ]
    for copy in reads:
        copy.start()
    for copy in inputs[1:]:
        copy.wait()
    wide = hidden[...].astype(F32)
    scaled = (wide * gain[...].astype(F32)[None, :]).astype(BF16)
    squares = jnp.sum(wide * wide, axis=1, keepdims=True)
    dt_rows = jnp.broadcast_to(dt_weight[...], (HEAD, dt_weight.shape[1]))
    first[...] = dot_nt(scaled, jnp.concatenate([x_weight[...], z_weight[...]], axis=0))
    last = dot_nt(scaled, jnp.concatenate([bc_weight[...], dt_rows], axis=0))
    second[...] = last
    turned = jnp.transpose(jnp.where(lanes_of((128, 128)) == HEAD + 1, squares, last))
    dt_line = jnp.broadcast_to(turned[HEAD : HEAD + 1], TILE)
    square_line = jnp.broadcast_to(turned[HEAD + 1 : HEAD + 2], TILE)
    square_high = rounded(square_line)
    rows = rows_of(TILE)
    upper = lanes_of(TILE) >= HEAD
    lines = jnp.where(rows == 4, dt_line, jnp.where(rows == 5, square_high, square_line - square_high))
    empty = jnp.zeros((SEQS, HEAD), F32)
    extra = [jnp.concatenate([empty, row], axis=1) for row in kept_rows(bc_history, accepted)]
    taps = jnp.concatenate([bc_kernel[...].astype(F32), jnp.zeros((4, HEAD), F32)], axis=0)
    taps = jnp.concatenate([empty, taps], axis=1)
    copies = []
    for j in range(TP):
        top = [first[pl.ds(TOKENS * j + t, SEQS, stride=PROPS), :] for t in range(PROPS)]
        low = [second[pl.ds(TOKENS * j + t, SEQS, stride=PROPS), :] for t in range(PROPS)]
        ending = jnp.where(rows < 4, taps, pltpu.roll(lines, (64 - 32 * j) % 128, 1))
        low = [jnp.where(upper, e, v) for e, v in zip([*extra, ending], low)]
        blocks[j] = jnp.concatenate(top + low, axis=0).astype(BF16)
        for g in range(NEAR_KV):
            copies.append(pltpu.make_async_copy(blocks.at[j], message.at[g * TP + j], leaving.at[g * TP + j]))
            copies[-1].start()
    for copy in reads + copies:
        copy.wait()


def pack_body(
    dt_bias,
    decay_log,
    skip_scale,
    accepted,
    first_state,
    weight,
    x_history,
    x_kernel,
    output_gain,
    kept_pack,
    sent,
):
    core = lax.axis_index("c")
    rows = rows_of(TILE)
    terms = [three_terms(number[0], TILE) for number in (dt_bias, decay_log, skip_scale)]
    gain_row = jnp.concatenate([jnp.zeros((1, HEAD), F32), output_gain[...].astype(F32)], axis=1)
    kernel = x_kernel[...].astype(F32)
    small = [widened(row) for row in kept_rows(x_history, accepted)]
    small = [jnp.where(core == 1, turned_half(tile), tile) for tile in small]
    small += [jnp.broadcast_to(widened(kernel[j : j + 1]), TILE) for j in range(4)]
    small = [small[0] + gain_row] + [a + b for a, b in zip(small[1:4], terms)] + small[4:]
    small.append(jnp.zeros(TILE, F32))
    kept_pack[0:SMALL, :] = jnp.concatenate([jnp.where(rows < HALF, tile, 0.0) for tile in small], axis=0).astype(BF16)
    for i in range(HALF):
        own = HALF * core + i
        kept_pack[SMALL + HEAD * i : SMALL + HEAD * (i + 1), :] = first_state[own].astype(BF16)
    sent[0:HEAD, :] = weight[...]
    small = [jnp.where(rows < HALF, 0.0, tile) for tile in small]
    blocks = [jnp.concatenate(small[2 * i : 2 * i + 2], axis=0) for i in range(SMALL // 16)]
    for i in range(HALF):
        other = HALF - HALF * core + i
        state = first_state[other]
        blocks += [state[16 * k : 16 * k + 16] for k in range(HEAD // 16)]
    blocks += [jnp.zeros((16, 128), F32)] * (weight.shape[1] // 128 - len(blocks))
    for i, block in enumerate(blocks):
        sent[HEAD : HEAD + 16, 128 * i : 128 * i + 128] = block.astype(BF16)


def summed_over_tp(arrived, place, start):
    total = arrived[place * TP, start : 2 * TOKENS, :].astype(F32)
    for k in range(1, TP):
        total = total + arrived[place * TP + k, start : 2 * TOKENS, :].astype(F32)
    return tiles(total)


def scale_line(ending):
    return lax.rsqrt((ending[5:6] + ending[6:7]) / D + EPSILON)


def mix_body(arrived, kept_pack, got, weight, message, columns, block_rows, leaving):
    core = lax.axis_index("c")
    pair = lax.axis_index("yl") * 2
    mine = lax.axis_index("tp")
    lanes = lanes_of(TILE)
    rows = rows_of(TILE)
    lower = lanes < HEAD
    first_rows = rows < HALF
    second_core = core == 1

    def halves(own, other):
        own = jnp.where(second_core, turned_half(own), own)
        other = jnp.where(second_core, other, turned_half(other))
        return jnp.where(rows_of(own.shape) < HALF, own, other)

    own = summed_over_tp(arrived, pair + core, 0)
    other = summed_over_tp(arrived, pair + 1 - core, 0)
    got_small = [got[HEAD : HEAD + 16, 128 * i : 128 * i + 128] for i in range(SMALL // 16)]
    small = tiles(kept_pack[0:SMALL, :].astype(F32) + jnp.concatenate(got_small, axis=0).astype(F32))
    gain = swapped(small[0])
    bias, decay, skip = [
        tile[:, HEAD : HEAD + 1] + tile[:, HEAD + 1 : HEAD + 2] + tile[:, HEAD + 2 : HEAD + 3] for tile in small[1:4]
    ]
    ending = own[7]
    lined = jnp.where(rows == 0, jnp.broadcast_to(scale_line(ending), TILE), ending)
    lined = jnp.where(rows == 1, jnp.broadcast_to(other[7][4:5], TILE), lined)
    columns[...] = jnp.transpose(lined)[HEAD : HEAD + TOKENS]
    rate = jnp.exp(decay)
    scale, step, cumulated = [], [], []
    total = jnp.zeros((SEQS, 1), F32)
    for t in range(PROPS):
        column = columns[pl.ds(t, SEQS, stride=PROPS), :]
        column = halves(column, column)
        scale.append(column[:, 0:1])
        raw = jnp.where(rows_of((SEQS, 1)) < HALF, column[:, 4:5], column[:, 1:2])
        step.append(softplus(rounded(scale[t] * raw) + bias))
        total = total - rate * step[t]
        cumulated.append(total)
    fresh = [rounded(scale[t] * halves(own[t], other[t])) for t in range(PROPS)]
    sums, extras = [], []
    for g in range(NEAR_KV):
        sums.append(summed_over_tp(arrived, g, TOKENS))
        extras.append(tiles(arrived[g * TP + mine, TOKENS : 2 * TOKENS, :].astype(F32)))

    def terms(left, right):
        window = [jnp.where(lower, swapped(extras[left][m]), extras[right][m]) for m in range(4)]
        new = [jnp.where(lower, sums[left][t], swapped(sums[right][t])) for t in range(PROPS)]
        taps = [window[3][j : j + 1] for j in range(4)]
        window = [halves(tile, tile) for tile in window[:3]]
        return convolved(window + [rounded(scale[t] * halves(new[t], new[t])) for t in range(PROPS)], taps)

    b_terms = terms(0, 1)
    c_terms = terms(2, 3)
    x_conv = convolved(small[0:3] + fresh, small[3:7])
    spans = range(SMALL // 16, (SMALL + HALF * HEAD) // 16)
    got_states = [got[HEAD : HEAD + 16, 128 * i : 128 * i + 128] for i in spans]
    states = jnp.concatenate([kept_pack[SMALL:, :], *got_states], axis=0)
    read = dot_nt(jnp.concatenate(c_terms, axis=0).astype(BF16), states)
    scaled = []
    squares = jnp.zeros(TILE, F32)
    quarter = lanes // TOKENS
    for t in range(PROPS):
        picked = jnp.zeros(TILE, F32)
        for k in range(SEQS // 2):
            picked = jnp.where(rows // 2 == k, read[8 * t : 8 * t + 8, 128 * k : 128 * k + 128], picked)
        picked = jnp.where(rows % 2 == 0, picked, swapped(picked))
        output = jnp.exp(cumulated[t]) * picked
        for r in range(t + 1):
            product = jnp.sum(c_terms[t] * b_terms[r], axis=1, keepdims=True)
            output = output + (jnp.exp(cumulated[t] - cumulated[r]) * step[r] * product) * x_conv[r]
        output = output + skip * x_conv[t]
        gated = output * silu(swapped(fresh[t]))
        both = jnp.where(lower, gated, swapped(turned_half(gated)))
        squares = jnp.where(quarter == t, jnp.sum(both * both, axis=1, keepdims=True), squares)
        gains = jnp.where(lower, gain, swapped(turned_half(gain)))
        scaled.append(both * gains)
    turns = []
    for d in range(4):
        turns += [row if d == 0 else pltpu.roll(row, 8 - 2 * d, 0) for row in scaled]
    turns = jnp.concatenate(turns, axis=0).astype(BF16)
    spot = jnp.where(first_rows & (lanes % TOKENS == rows), squares, 0.0)
    square_line = jnp.sum(spot, axis=0, keepdims=True)
    high = rounded(square_line)
    lines = jnp.where(rows % 2 == 0, high, square_line - high)
    copies = []
    for i in range(weight.shape[1] // 256):
        cut = slice(256 * i, 256 * (i + 1))
        both_weights = jnp.concatenate([weight[:, cut], got[0:HEAD, cut]], axis=0)
        product = jnp.dot(turns, both_weights, preferred_element_type=F32)
        pieces = []
        for half in range(2):
            block = product[:, 128 * half : 128 * (half + 1)]
            spots = []
            for d in range(4):
                spot = None
                for t in range(PROPS):
                    piece = block[32 * d + 8 * t : 32 * d + 8 * t + 8]
                    piece = piece if t == d else pltpu.roll(piece, (32 * (t - d)) % 128, 1)
                    spot = piece if t == 0 else jnp.where(quarter == t, piece, spot)
                spots.append(spot)
            pieces += [
                jnp.where(rows < 4, spots[0], jnp.where(rows < 6, lines, spots[1])),
                jnp.where(rows < 2, spots[1], jnp.where(rows < 4, lines, spots[2])),
                jnp.where((rows >= 2) & (rows < 6), spots[3], lines),
            ]
        block_rows[48 * i : 48 * (i + 1), :] = jnp.concatenate(pieces, axis=0).astype(BF16)
        if i % 4 == 3:
            part = pl.ds(48 * (i - 3), 192)
            copies.append(pltpu.make_async_copy(block_rows.at[part], message.at[part], leaving.at[i // 4]))
            copies[-1].start()
    for copy in copies:
        copy.wait()


def state_body(
    dt_bias,
    decay_log,
    accepted,
    arrived,
    first_state,
    x_kernel,
    x_history,
    new_states,
    x_window,
    bc_window,
    columns,
):
    place = lax.axis_index(("yl", "c"))
    mine = lax.axis_index("tp")
    lanes = lanes_of(TILE)
    lower = lanes < HEAD
    own = summed_over_tp(arrived, place, 0)
    ending = own[7]
    lined = jnp.where(rows_of(TILE) == 0, jnp.broadcast_to(scale_line(ending), TILE), ending)
    columns[...] = jnp.transpose(lined)[HEAD : HEAD + TOKENS]
    bias = dt_bias[0]
    rate = jnp.exp(jnp.full((SEQS, 1), decay_log[0], F32))
    scale, step = [], []
    for t in range(PROPS):
        column = columns[pl.ds(t, SEQS, stride=PROPS), :]
        scale.append(column[:, 0:1])
        step.append(softplus(rounded(scale[t] * column[:, 4:5]) + bias))
    fresh = [rounded(scale[t] * own[t]) for t in range(PROPS)]
    sums = [summed_over_tp(arrived, g, TOKENS) for g in range(2)]
    extras = [tiles(arrived[g * TP + mine, TOKENS : 2 * TOKENS, :].astype(F32)) for g in range(2)]
    window = [jnp.where(lower, swapped(extras[0][m]), extras[1][m]) for m in range(4)]
    new = [rounded(scale[t] * jnp.where(lower, sums[0][t], swapped(sums[1][t]))) for t in range(PROPS)]
    b_terms = convolved(window[:3] + new, [window[3][j : j + 1] for j in range(4)])
    kept = kept_rows(x_history, accepted)
    kernel = widened(x_kernel[...].astype(F32))
    x_conv = convolved([widened(row) for row in kept] + fresh, [kernel[j : j + 1] for j in range(4)])
    inputs = [x_conv[t] * step[t] for t in range(PROPS)]
    turned = jnp.transpose(jnp.concatenate(inputs + [jnp.zeros((128 - TOKENS, 128), F32)], axis=0))[:HEAD]
    decay = [jnp.broadcast_to(jnp.exp(-rate * step[t]), TILE) for t in range(PROPS)]
    for s in range(SEQS):
        state = first_state[s]
        new_states[s, 0, 0] = state
        for t in range(PROPS):
            at = 8 * t + s
            state = state * decay[t][s : s + 1, :] + turned[:, at : at + 1] * b_terms[t][s : s + 1, :]
            new_states[s, t + 1, 0] = state
    own_extra = tiles(arrived[place * TP + mine, TOKENS : 2 * TOKENS, :].astype(F32))
    for m in range(3):
        x_window[m] = kept[m].astype(BF16)
        bc_window[m] = swapped(own_extra[m])[:, :HEAD].astype(BF16)
    for t in range(PROPS):
        x_window[3 + t] = fresh[t][:, :HEAD].astype(BF16)
        bc_window[3 + t] = (scale[t] * own[4 + t])[:, :HEAD].astype(BF16)


def finish_body(arrived, mixed, total, placed):
    step = 8 * LINES
    running = arrived[0:step, :].astype(F32)
    for i in range(1, arrived.shape[0] // step):
        running = running + arrived[step * i : step * (i + 1), :].astype(F32)
    total[...] = running
    sums = []
    for c in range(2):
        start = LINES * c
        part = total[start : start + LINES, :]
        for i in range(1, 4):
            part = part + total[2 * LINES * i + start : 2 * LINES * i + start + LINES, :]
        sums.append(part)
    summed = jnp.concatenate([part[:HALF] for part in sums], axis=0)
    means = [jnp.broadcast_to((part[4:5] + part[5:6]) / INNER, (HALF, 128)) for part in sums]
    mean = jnp.concatenate(means, axis=0)
    lanes = lanes_of(TILE)
    rows = rows_of(TILE)
    for t in range(PROPS):
        own = jnp.sum(jnp.where(lanes == TOKENS * t + rows % HALF, mean, 0.0), axis=1, keepdims=True)
        moved = summed if t == 0 else pltpu.roll(summed, 128 - TOKENS * t, 1)
        placed[pl.ds(t, SEQS, stride=PROPS), :] = lax.rsqrt(own + EPSILON) * moved
    mixed[...] = placed[...][:, :TOKENS].astype(BF16)


def smem():
    return pl.BlockSpec(memory_space=pltpu.SMEM)


def vmem():
    return pl.BlockSpec(memory_space=pltpu.VMEM)


def far_memory():
    return pl.BlockSpec(memory_space=pltpu.HBM)


def near_memory(value):
    return pltpu.with_memory_space_constraint(value, pltpu.VMEM)


def local(
    hidden,
    input_gain,
    x_weight,
    z_weight,
    bc_weight,
    dt_weight,
    x_kernel,
    bc_kernel,
    dt_bias,
    decay_log,
    skip_scale,
    output_gain,
    output_weight,
    saved_states,
    x_history,
    bc_history,
    accepted,
):
    shape = jax.ShapeDtypeStruct
    held = pltpu.VMEM
    lines = KV_SIZE * LINES
    x_rows = jnp.transpose(x_history, (1, 0, 2))
    bc_rows = jnp.transpose(bc_history, (1, 0, 2))
    pack_rows = SMALL + HALF * HEAD
    near, first_state = pl.pallas_call(
        project_body,
        out_shape=(shape((TP * NEAR_KV, 2 * TOKENS, 128), BF16), held((SEQS, HEAD, STATE), F32)),
        in_specs=[far_memory()] * 10,
        out_specs=(far_memory(), vmem()),
        scratch_shapes=[
            pltpu.SMEM(accepted.shape, jnp.int32),
            pltpu.VMEM(accepted.shape, jnp.int32),
            pltpu.VMEM(hidden.shape, BF16),
            pltpu.VMEM(x_weight.T.shape, BF16),
            pltpu.VMEM(z_weight.T.shape, BF16),
            pltpu.VMEM(bc_weight.T.shape, BF16),
            pltpu.VMEM(input_gain.shape, BF16),
            pltpu.VMEM(dt_weight.T.shape, BF16),
            pltpu.VMEM(bc_rows.shape, BF16),
            pltpu.VMEM(bc_kernel.shape, BF16),
            pltpu.VMEM((128, 128), F32),
            pltpu.VMEM((128, 128), F32),
            pltpu.VMEM((TP, 2 * TOKENS, 128), BF16),
            pltpu.SemaphoreType.DMA((10,)),
            pltpu.SemaphoreType.DMA((SEQS,)),
            pltpu.SemaphoreType.DMA((TP * NEAR_KV,)),
        ],
    )(accepted, saved_states, hidden, x_weight.T, z_weight.T, bc_weight.T, input_gain, dt_weight.T, bc_rows, bc_kernel)
    first_state = near_memory(first_state)
    output_weight = near_memory(output_weight)
    arrived = near_memory(lax.all_to_all(near, NEAR, 0, 0, tiled=True))
    kept_pack, sent = pl.pallas_call(
        pack_body,
        out_shape=(held((pack_rows, 128), BF16), held((HEAD + 16, output_weight.shape[1]), BF16)),
        in_specs=[smem()] * 3 + [vmem()] * 6,
        out_specs=(vmem(),) * 2,
        cost_estimate=pl.CostEstimate(flops=4_000_000, bytes_accessed=3_000_000, transcendentals=0),
    )(
        dt_bias,
        decay_log,
        skip_scale,
        near_memory(accepted),
        first_state,
        output_weight,
        near_memory(x_rows),
        near_memory(x_kernel),
        near_memory(output_gain.reshape(1, HEAD)),
    )
    got = lax.ppermute(sent, "c", [(0, 1), (1, 0)])
    far = pl.pallas_call(
        mix_body,
        out_shape=shape((lines, 128), BF16),
        in_specs=[vmem()] * 4,
        out_specs=far_memory(),
        scratch_shapes=[pltpu.VMEM((TOKENS, 8), F32), pltpu.VMEM((lines, 128), BF16), pltpu.SemaphoreType.DMA((4,))],
    )(arrived, near_memory(kept_pack), near_memory(got), output_weight)
    landed = lax.all_to_all(far.reshape(KV_SIZE, LINES // 2, 2, 128), KV, 0, 0, tiled=True)
    landed = near_memory(landed.reshape(lines, 128))
    new_states, x_window, bc_window = pl.pallas_call(
        state_body,
        out_shape=(
            shape((SEQS, PROPS + 1, 1, HEAD, STATE), F32),
            shape((7, SEQS, HEAD), BF16),
            shape((7, SEQS, HEAD), BF16),
        ),
        in_specs=[smem()] * 2 + [vmem()] * 5,
        out_specs=(vmem(),) * 3,
        scratch_shapes=[pltpu.VMEM((TOKENS, 8), F32)],
        cost_estimate=pl.CostEstimate(flops=4_000_000, bytes_accessed=3_000_000, transcendentals=0),
    )(
        dt_bias,
        decay_log,
        accepted,
        arrived,
        first_state,
        x_kernel,
        x_rows,
    )
    mixed = pl.pallas_call(
        finish_body,
        out_shape=shape((TOKENS, TOKENS), BF16),
        in_specs=[vmem()],
        out_specs=vmem(),
        scratch_shapes=[pltpu.VMEM((8 * LINES, 128), F32), pltpu.VMEM((TOKENS, 128), F32)],
    )(landed)
    return (mixed, new_states, jnp.transpose(x_window, (1, 0, 2)), jnp.transpose(bc_window, (1, 0, 2)))


def solution(mesh):
    split = Mesh(mesh.devices.reshape(8, 4, 2, 2, mesh.shape["tp"]), ("z", "yh", "yl", "c", "tp"))
    return jax.shard_map(
        local,
        mesh=split,
        in_specs=(
            P(None, "tp"),
            P("tp"),
            P("tp", KV),
            P("tp", KV),
            P("tp", KV),
            P("tp", KV),
            P(None, KV),
            P(None, KV),
            P(KV),
            P(KV),
            P(KV),
            P(KV),
            P(KV, None),
            P("tp", None, KV, None, None),
            P("tp", None, KV),
            P("tp", None, KV),
            P("tp"),
        ),
        out_specs=(
            P("tp", KV),
            P("tp", None, KV, None, None),
            P("tp", None, KV),
            P("tp", None, KV),
        ),
        check_vma=False,
    )
```

```python
import jax
import jax.numpy as jnp
from jax import lax
from jax.experimental import pallas as pl
from jax.experimental.pallas import tpu as pltpu
from jax.sharding import Mesh
from jax.sharding import PartitionSpec as P


D = 4096
PROPS = 4
INNER = 8192
KV = ("z", "yh", "yl", "c")
NEAR = ("yl", "c", "tp")
EPSILON = 1e-05
TP = 4
NEAR_KV = 4
KV_SIZE = 128
SEQS = 8
HALF = 4
TOKENS = 32
HEAD = 64
STATE = 128
LINES = 6
TILE = (8, 128)
FAR_FIRST = 88
NEAR_FIRST = 0
SMALL = 64

F32 = jnp.float32
BF16 = jnp.bfloat16


def rounded(value):
    return value.astype(BF16).astype(F32)


def lanes_of(shape):
    return lax.broadcasted_iota(jnp.int32, shape, len(shape) - 1)


def rows_of(shape):
    return lax.broadcasted_iota(jnp.int32, shape, len(shape) - 2)


def dot_nt(a, b):
    return lax.dot_general(a, b, (((1,), (1,)), ((), ())), preferred_element_type=F32)


def silu(v):
    return v / (1.0 + jnp.exp(-v))


def softplus(v):
    return jnp.maximum(v, 0.0) + jnp.log1p(jnp.exp(-jnp.abs(v)))


def tiles(value):
    return [value[8 * i : 8 * i + 8] for i in range(value.shape[0] // 8)]


def swapped(tile):
    return pltpu.roll(tile, HEAD, 1)


def turned_half(tile):
    return pltpu.roll(tile, HALF, 0)


def widened(tile):
    return jnp.concatenate([tile, jnp.zeros(tile.shape, tile.dtype)], axis=1)


def kept_rows(history, accepted):
    line = jnp.broadcast_to(accepted[...].astype(F32)[None, :], (SEQS, SEQS))
    own = lanes_of((SEQS, SEQS)) == rows_of((SEQS, SEQS))
    column = jnp.sum(jnp.where(own, line, 0.0), axis=1, keepdims=True)
    whole = [history[i].astype(F32) for i in range(7)]
    kept = []
    for m in range(3):
        row = whole[m]
        for a in range(1, PROPS + 1):
            row = jnp.where(column == float(a), whole[m + a], row)
        kept.append(row)
    return kept


def convolved(window, taps):
    results = []
    for t in range(PROPS):
        running = window[t] * taps[0]
        for j in range(1, 4):
            running = running + window[t + j] * taps[j]
        results.append(silu(running))
    return results


def three_terms(value, shape):
    value = jnp.broadcast_to(value, shape)
    high = rounded(value)
    middle = rounded(value - high)
    lanes = lanes_of(shape)
    low = value - high - middle
    return jnp.where(lanes == HEAD, high, jnp.where(lanes == HEAD + 1, middle, jnp.where(lanes == HEAD + 2, low, 0.0)))


def project_body(
    accepted_far,
    saved,
    hidden_far,
    x_weight_far,
    z_weight_far,
    bc_weight_far,
    gain_far,
    dt_weight_far,
    bc_history_far,
    bc_kernel_far,
    message,
    first_state,
    chosen,
    accepted,
    hidden,
    x_weight,
    z_weight,
    bc_weight,
    gain,
    dt_weight,
    bc_history,
    bc_kernel,
    first,
    second,
    blocks,
    coming,
    reading,
    leaving,
):
    sources = [
        accepted_far,
        hidden_far,
        x_weight_far,
        z_weight_far,
        bc_weight_far,
        gain_far,
        dt_weight_far,
        bc_history_far,
        bc_kernel_far,
        accepted_far,
    ]
    targets = [chosen, hidden, x_weight, z_weight, bc_weight, gain, dt_weight, bc_history, bc_kernel, accepted]
    inputs = [pltpu.make_async_copy(a, b, coming.at[i]) for i, (a, b) in enumerate(zip(sources, targets))]
    for copy in inputs:
        copy.start()
    inputs[0].wait()
    reads = [
        pltpu.make_async_copy(saved.at[s, chosen[s], 0], first_state.at[s], reading.at[s]) for s in range(SEQS)
    ]
    for copy in reads:
        copy.start()
    for copy in inputs[1:]:
        copy.wait()
    wide = hidden[...].astype(F32)
    scaled = (wide * gain[...].astype(F32)[None, :]).astype(BF16)
    squares = jnp.sum(wide * wide, axis=1, keepdims=True)
    dt_rows = jnp.broadcast_to(dt_weight[...], (HEAD, dt_weight.shape[1]))
    first[...] = dot_nt(scaled, jnp.concatenate([x_weight[...], z_weight[...]], axis=0))
    last = dot_nt(scaled, jnp.concatenate([bc_weight[...], dt_rows], axis=0))
    second[...] = last
    turned = jnp.transpose(jnp.where(lanes_of((128, 128)) == HEAD + 1, squares, last))
    dt_line = jnp.broadcast_to(turned[HEAD : HEAD + 1], TILE)
    square_line = jnp.broadcast_to(turned[HEAD + 1 : HEAD + 2], TILE)
    square_high = rounded(square_line)
    rows = rows_of(TILE)
    upper = lanes_of(TILE) >= HEAD
    lines = jnp.where(rows == 4, dt_line, jnp.where(rows == 5, square_high, square_line - square_high))
    empty = jnp.zeros((SEQS, HEAD), F32)
    extra = [jnp.concatenate([empty, row], axis=1) for row in kept_rows(bc_history, accepted)]
    taps = jnp.concatenate([bc_kernel[...].astype(F32), jnp.zeros((4, HEAD), F32)], axis=0)
    taps = jnp.concatenate([empty, taps], axis=1)
    copies = []
    for j in range(TP):
        top = [first[pl.ds(TOKENS * j + t, SEQS, stride=PROPS), :] for t in range(PROPS)]
        low = [second[pl.ds(TOKENS * j + t, SEQS, stride=PROPS), :] for t in range(PROPS)]
        ending = jnp.where(rows < 4, taps, pltpu.roll(lines, (64 - 32 * j) % 128, 1))
        low = [jnp.where(upper, e, v) for e, v in zip([*extra, ending], low)]
        blocks[j] = jnp.concatenate(top + low, axis=0).astype(BF16)
        for g in range(NEAR_KV):
            copies.append(pltpu.make_async_copy(blocks.at[j], message.at[g * TP + (j - NEAR_FIRST) % TP], leaving.at[g * TP + j]))
            copies[-1].start()
    for copy in reads + copies:
        copy.wait()


def pack_body(
    dt_bias,
    decay_log,
    skip_scale,
    accepted,
    first_state,
    weight,
    x_history,
    x_kernel,
    output_gain,
    kept_pack,
    sent,
):
    core = lax.axis_index("c")
    rows = rows_of(TILE)
    terms = [three_terms(number[0], TILE) for number in (dt_bias, decay_log, skip_scale)]
    gain_row = jnp.concatenate([jnp.zeros((1, HEAD), F32), output_gain[...].astype(F32)], axis=1)
    kernel = x_kernel[...].astype(F32)
    small = [widened(row) for row in kept_rows(x_history, accepted)]
    small = [jnp.where(core == 1, turned_half(tile), tile) for tile in small]
    small += [jnp.broadcast_to(widened(kernel[j : j + 1]), TILE) for j in range(4)]
    small = [small[0] + gain_row] + [a + b for a, b in zip(small[1:4], terms)] + small[4:]
    small.append(jnp.zeros(TILE, F32))
    kept_pack[0:SMALL, :] = jnp.concatenate([jnp.where(rows < HALF, tile, 0.0) for tile in small], axis=0).astype(BF16)
    for i in range(HALF):
        own = HALF * core + i
        kept_pack[SMALL + HEAD * i : SMALL + HEAD * (i + 1), :] = first_state[own].astype(BF16)
    sent[0:HEAD, :] = weight[...]
    small = [jnp.where(rows < HALF, 0.0, tile) for tile in small]
    blocks = [jnp.concatenate(small[2 * i : 2 * i + 2], axis=0) for i in range(SMALL // 16)]
    for i in range(HALF):
        other = HALF - HALF * core + i
        state = first_state[other]
        blocks += [state[16 * k : 16 * k + 16] for k in range(HEAD // 16)]
    blocks += [jnp.zeros((16, 128), F32)] * (weight.shape[1] // 128 - len(blocks))
    for i, block in enumerate(blocks):
        sent[HEAD : HEAD + 16, 128 * i : 128 * i + 128] = block.astype(BF16)


def summed_over_tp(arrived, place, start):
    total = arrived[place * TP, start : 2 * TOKENS, :].astype(F32)
    for k in range(1, TP):
        total = total + arrived[place * TP + k, start : 2 * TOKENS, :].astype(F32)
    return tiles(total)


def scale_line(ending):
    return lax.rsqrt((ending[5:6] + ending[6:7]) / D + EPSILON)


def mix_body(arrived, kept_pack, got, weight, message, columns, block_rows, leaving):
    core = lax.axis_index("c")
    pair = lax.axis_index("yl") * 2
    mine = (lax.axis_index("tp") + TP - NEAR_FIRST) % TP
    lanes = lanes_of(TILE)
    rows = rows_of(TILE)
    lower = lanes < HEAD
    first_rows = rows < HALF
    second_core = core == 1

    def halves(own, other):
        own = jnp.where(second_core, turned_half(own), own)
        other = jnp.where(second_core, other, turned_half(other))
        return jnp.where(rows_of(own.shape) < HALF, own, other)

    own = summed_over_tp(arrived, pair + core, 0)
    other = summed_over_tp(arrived, pair + 1 - core, 0)
    got_small = [got[HEAD : HEAD + 16, 128 * i : 128 * i + 128] for i in range(SMALL // 16)]
    small = tiles(kept_pack[0:SMALL, :].astype(F32) + jnp.concatenate(got_small, axis=0).astype(F32))
    gain = swapped(small[0])
    bias, decay, skip = [
        tile[:, HEAD : HEAD + 1] + tile[:, HEAD + 1 : HEAD + 2] + tile[:, HEAD + 2 : HEAD + 3] for tile in small[1:4]
    ]
    ending = own[7]
    lined = jnp.where(rows == 0, jnp.broadcast_to(scale_line(ending), TILE), ending)
    lined = jnp.where(rows == 1, jnp.broadcast_to(other[7][4:5], TILE), lined)
    columns[...] = jnp.transpose(lined)[HEAD : HEAD + TOKENS]
    rate = jnp.exp(decay)
    scale, step, cumulated = [], [], []
    total = jnp.zeros((SEQS, 1), F32)
    for t in range(PROPS):
        column = columns[pl.ds(t, SEQS, stride=PROPS), :]
        column = halves(column, column)
        scale.append(column[:, 0:1])
        raw = jnp.where(rows_of((SEQS, 1)) < HALF, column[:, 4:5], column[:, 1:2])
        step.append(softplus(rounded(scale[t] * raw) + bias))
        total = total - rate * step[t]
        cumulated.append(total)
    fresh = [rounded(scale[t] * halves(own[t], other[t])) for t in range(PROPS)]
    sums, extras = [], []
    for g in range(NEAR_KV):
        sums.append(summed_over_tp(arrived, g, TOKENS))
        extras.append(tiles(arrived[g * TP + mine, TOKENS : 2 * TOKENS, :].astype(F32)))

    def terms(left, right):
        window = [jnp.where(lower, swapped(extras[left][m]), extras[right][m]) for m in range(4)]
        new = [jnp.where(lower, sums[left][t], swapped(sums[right][t])) for t in range(PROPS)]
        taps = [window[3][j : j + 1] for j in range(4)]
        window = [halves(tile, tile) for tile in window[:3]]
        return convolved(window + [rounded(scale[t] * halves(new[t], new[t])) for t in range(PROPS)], taps)

    b_terms = terms(0, 1)
    c_terms = terms(2, 3)
    x_conv = convolved(small[0:3] + fresh, small[3:7])
    spans = range(SMALL // 16, (SMALL + HALF * HEAD) // 16)
    got_states = [got[HEAD : HEAD + 16, 128 * i : 128 * i + 128] for i in spans]
    states = jnp.concatenate([kept_pack[SMALL:, :], *got_states], axis=0)
    read = dot_nt(jnp.concatenate(c_terms, axis=0).astype(BF16), states)
    scaled = []
    squares = jnp.zeros(TILE, F32)
    quarter = lanes // TOKENS
    for t in range(PROPS):
        picked = jnp.zeros(TILE, F32)
        for k in range(SEQS // 2):
            picked = jnp.where(rows // 2 == k, read[8 * t : 8 * t + 8, 128 * k : 128 * k + 128], picked)
        picked = jnp.where(rows % 2 == 0, picked, swapped(picked))
        output = jnp.exp(cumulated[t]) * picked
        for r in range(t + 1):
            product = jnp.sum(c_terms[t] * b_terms[r], axis=1, keepdims=True)
            output = output + (jnp.exp(cumulated[t] - cumulated[r]) * step[r] * product) * x_conv[r]
        output = output + skip * x_conv[t]
        gated = output * silu(swapped(fresh[t]))
        both = jnp.where(lower, gated, swapped(turned_half(gated)))
        squares = jnp.where(quarter == t, jnp.sum(both * both, axis=1, keepdims=True), squares)
        gains = jnp.where(lower, gain, swapped(turned_half(gain)))
        scaled.append(both * gains)
    turns = []
    for d in range(4):
        turns += [row if d == 0 else pltpu.roll(row, 8 - 2 * d, 0) for row in scaled]
    turns = jnp.concatenate(turns, axis=0).astype(BF16)
    spot = jnp.where(first_rows & (lanes % TOKENS == rows), squares, 0.0)
    square_line = jnp.sum(spot, axis=0, keepdims=True)
    high = rounded(square_line)
    lines = jnp.where(rows % 2 == 0, high, square_line - high)
    copies = []
    chunks = weight.shape[1] // 256
    for i in range(chunks):
        spot = (i + FAR_FIRST // 8) % chunks
        cut = slice(256 * spot, 256 * (spot + 1))
        both_weights = jnp.concatenate([weight[:, cut], got[0:HEAD, cut]], axis=0)
        product = jnp.dot(turns, both_weights, preferred_element_type=F32)
        pieces = []
        for half in range(2):
            block = product[:, 128 * half : 128 * (half + 1)]
            spots = []
            for d in range(4):
                spot = None
                for t in range(PROPS):
                    piece = block[32 * d + 8 * t : 32 * d + 8 * t + 8]
                    piece = piece if t == d else pltpu.roll(piece, (32 * (t - d)) % 128, 1)
                    spot = piece if t == 0 else jnp.where(quarter == t, piece, spot)
                spots.append(spot)
            pieces += [
                jnp.where(rows < 4, spots[0], jnp.where(rows < 6, lines, spots[1])),
                jnp.where(rows < 2, spots[1], jnp.where(rows < 4, lines, spots[2])),
                jnp.where((rows >= 2) & (rows < 6), spots[3], lines),
            ]
        block_rows[48 * i : 48 * (i + 1), :] = jnp.concatenate(pieces, axis=0).astype(BF16)
        if i % 4 == 3:
            part = pl.ds(48 * (i - 3), 192)
            copies.append(pltpu.make_async_copy(block_rows.at[part], message.at[part], leaving.at[i // 4]))
            copies[-1].start()
    for copy in copies:
        copy.wait()


def state_body(
    dt_bias,
    decay_log,
    accepted,
    arrived,
    first_state,
    x_kernel,
    x_history,
    new_states,
    x_window,
    bc_window,
    columns,
):
    place = lax.axis_index(("yl", "c"))
    mine = (lax.axis_index("tp") + TP - NEAR_FIRST) % TP
    lanes = lanes_of(TILE)
    lower = lanes < HEAD
    own = summed_over_tp(arrived, place, 0)
    ending = own[7]
    lined = jnp.where(rows_of(TILE) == 0, jnp.broadcast_to(scale_line(ending), TILE), ending)
    columns[...] = jnp.transpose(lined)[HEAD : HEAD + TOKENS]
    bias = dt_bias[0]
    rate = jnp.exp(jnp.full((SEQS, 1), decay_log[0], F32))
    scale, step = [], []
    for t in range(PROPS):
        column = columns[pl.ds(t, SEQS, stride=PROPS), :]
        scale.append(column[:, 0:1])
        step.append(softplus(rounded(scale[t] * column[:, 4:5]) + bias))
    fresh = [rounded(scale[t] * own[t]) for t in range(PROPS)]
    sums = [summed_over_tp(arrived, g, TOKENS) for g in range(2)]
    extras = [tiles(arrived[g * TP + mine, TOKENS : 2 * TOKENS, :].astype(F32)) for g in range(2)]
    window = [jnp.where(lower, swapped(extras[0][m]), extras[1][m]) for m in range(4)]
    new = [rounded(scale[t] * jnp.where(lower, sums[0][t], swapped(sums[1][t]))) for t in range(PROPS)]
    b_terms = convolved(window[:3] + new, [window[3][j : j + 1] for j in range(4)])
    kept = kept_rows(x_history, accepted)
    kernel = widened(x_kernel[...].astype(F32))
    x_conv = convolved([widened(row) for row in kept] + fresh, [kernel[j : j + 1] for j in range(4)])
    inputs = [x_conv[t] * step[t] for t in range(PROPS)]
    turned = jnp.transpose(jnp.concatenate(inputs + [jnp.zeros((128 - TOKENS, 128), F32)], axis=0))[:HEAD]
    decay = [jnp.broadcast_to(jnp.exp(-rate * step[t]), TILE) for t in range(PROPS)]
    for s in range(SEQS):
        state = first_state[s]
        new_states[s, 0, 0] = state
        for t in range(PROPS):
            at = 8 * t + s
            state = state * decay[t][s : s + 1, :] + turned[:, at : at + 1] * b_terms[t][s : s + 1, :]
            new_states[s, t + 1, 0] = state
    own_extra = tiles(arrived[place * TP + mine, TOKENS : 2 * TOKENS, :].astype(F32))
    for m in range(3):
        x_window[m] = kept[m].astype(BF16)
        bc_window[m] = swapped(own_extra[m])[:, :HEAD].astype(BF16)
    for t in range(PROPS):
        x_window[3 + t] = fresh[t][:, :HEAD].astype(BF16)
        bc_window[3 + t] = (scale[t] * own[4 + t])[:, :HEAD].astype(BF16)


def finish_body(arrived, mixed, total, placed):
    step = 8 * LINES
    running = arrived[0:step, :].astype(F32)
    for i in range(1, arrived.shape[0] // step):
        running = running + arrived[step * i : step * (i + 1), :].astype(F32)
    total[...] = running
    sums = []
    for c in range(2):
        start = LINES * c
        part = total[start : start + LINES, :]
        for i in range(1, 4):
            part = part + total[2 * LINES * i + start : 2 * LINES * i + start + LINES, :]
        sums.append(part)
    summed = jnp.concatenate([part[:HALF] for part in sums], axis=0)
    means = [jnp.broadcast_to((part[4:5] + part[5:6]) / INNER, (HALF, 128)) for part in sums]
    mean = jnp.concatenate(means, axis=0)
    lanes = lanes_of(TILE)
    rows = rows_of(TILE)
    for t in range(PROPS):
        own = jnp.sum(jnp.where(lanes == TOKENS * t + rows % HALF, mean, 0.0), axis=1, keepdims=True)
        moved = summed if t == 0 else pltpu.roll(summed, 128 - TOKENS * t, 1)
        placed[pl.ds(t, SEQS, stride=PROPS), :] = lax.rsqrt(own + EPSILON) * moved
    mixed[...] = placed[...][:, :TOKENS].astype(BF16)


def smem():
    return pl.BlockSpec(memory_space=pltpu.SMEM)


def vmem():
    return pl.BlockSpec(memory_space=pltpu.VMEM)


def far_memory():
    return pl.BlockSpec(memory_space=pltpu.HBM)


def near_memory(value):
    return pltpu.with_memory_space_constraint(value, pltpu.VMEM)


def local(
    hidden,
    input_gain,
    x_weight,
    z_weight,
    bc_weight,
    dt_weight,
    x_kernel,
    bc_kernel,
    dt_bias,
    decay_log,
    skip_scale,
    output_gain,
    output_weight,
    saved_states,
    x_history,
    bc_history,
    accepted,
):
    shape = jax.ShapeDtypeStruct
    held = pltpu.VMEM
    lines = KV_SIZE * LINES
    x_rows = jnp.transpose(x_history, (1, 0, 2))
    bc_rows = jnp.transpose(bc_history, (1, 0, 2))
    pack_rows = SMALL + HALF * HEAD
    near, first_state = pl.pallas_call(
        project_body,
        out_shape=(shape((TP * NEAR_KV, 2 * TOKENS, 128), BF16), held((SEQS, HEAD, STATE), F32)),
        in_specs=[far_memory()] * 10,
        out_specs=(far_memory(), vmem()),
        scratch_shapes=[
            pltpu.SMEM(accepted.shape, jnp.int32),
            pltpu.VMEM(accepted.shape, jnp.int32),
            pltpu.VMEM(hidden.shape, BF16),
            pltpu.VMEM(x_weight.T.shape, BF16),
            pltpu.VMEM(z_weight.T.shape, BF16),
            pltpu.VMEM(bc_weight.T.shape, BF16),
            pltpu.VMEM(input_gain.shape, BF16),
            pltpu.VMEM(dt_weight.T.shape, BF16),
            pltpu.VMEM(bc_rows.shape, BF16),
            pltpu.VMEM(bc_kernel.shape, BF16),
            pltpu.VMEM((128, 128), F32),
            pltpu.VMEM((128, 128), F32),
            pltpu.VMEM((TP, 2 * TOKENS, 128), BF16),
            pltpu.SemaphoreType.DMA((10,)),
            pltpu.SemaphoreType.DMA((SEQS,)),
            pltpu.SemaphoreType.DMA((TP * NEAR_KV,)),
        ],
    )(accepted, saved_states, hidden, x_weight.T, z_weight.T, bc_weight.T, input_gain, dt_weight.T, bc_rows, bc_kernel)
    first_state = near_memory(first_state)
    output_weight = near_memory(output_weight)
    order = [[g * TP + (k + NEAR_FIRST) % TP for g in range(NEAR_KV) for k in range(TP)]]
    arrived = near_memory(lax.all_to_all(near, NEAR, 0, 0, tiled=True, axis_index_groups=order))
    kept_pack, sent = pl.pallas_call(
        pack_body,
        out_shape=(held((pack_rows, 128), BF16), held((HEAD + 16, output_weight.shape[1]), BF16)),
        in_specs=[smem()] * 3 + [vmem()] * 6,
        out_specs=(vmem(),) * 2,
        cost_estimate=pl.CostEstimate(flops=4_000_000, bytes_accessed=3_000_000, transcendentals=0),
    )(
        dt_bias,
        decay_log,
        skip_scale,
        near_memory(accepted),
        first_state,
        output_weight,
        near_memory(x_rows),
        near_memory(x_kernel),
        near_memory(output_gain.reshape(1, HEAD)),
    )
    got = lax.ppermute(sent, "c", [(0, 1), (1, 0)])
    far = pl.pallas_call(
        mix_body,
        out_shape=shape((lines, 128), BF16),
        in_specs=[vmem()] * 4,
        out_specs=far_memory(),
        scratch_shapes=[pltpu.VMEM((TOKENS, 8), F32), pltpu.VMEM((lines, 128), BF16), pltpu.SemaphoreType.DMA((4,))],
    )(arrived, near_memory(kept_pack), near_memory(got), output_weight)
    order = [[(i + FAR_FIRST) % KV_SIZE for i in range(KV_SIZE)]]
    far = far.reshape(KV_SIZE, LINES // 2, 2, 128)
    landed = lax.all_to_all(far, KV, 0, 0, tiled=True, axis_index_groups=order)
    landed = near_memory(landed.reshape(lines, 128))
    new_states, x_window, bc_window = pl.pallas_call(
        state_body,
        out_shape=(
            shape((SEQS, PROPS + 1, 1, HEAD, STATE), F32),
            shape((7, SEQS, HEAD), BF16),
            shape((7, SEQS, HEAD), BF16),
        ),
        in_specs=[smem()] * 2 + [vmem()] * 5,
        out_specs=(vmem(),) * 3,
        scratch_shapes=[pltpu.VMEM((TOKENS, 8), F32)],
        cost_estimate=pl.CostEstimate(flops=4_000_000, bytes_accessed=3_000_000, transcendentals=0),
    )(
        dt_bias,
        decay_log,
        accepted,
        arrived,
        first_state,
        x_kernel,
        x_rows,
    )
    mixed = pl.pallas_call(
        finish_body,
        out_shape=shape((TOKENS, TOKENS), BF16),
        in_specs=[vmem()],
        out_specs=vmem(),
        scratch_shapes=[pltpu.VMEM((8 * LINES, 128), F32), pltpu.VMEM((TOKENS, 128), F32)],
    )(landed)
    return (mixed, new_states, jnp.transpose(x_window, (1, 0, 2)), jnp.transpose(bc_window, (1, 0, 2)))


def solution(mesh):
    split = Mesh(mesh.devices.reshape(8, 4, 2, 2, mesh.shape["tp"]), ("z", "yh", "yl", "c", "tp"))
    return jax.shard_map(
        local,
        mesh=split,
        in_specs=(
            P(None, "tp"),
            P("tp"),
            P("tp", KV),
            P("tp", KV),
            P("tp", KV),
            P("tp", KV),
            P(None, KV),
            P(None, KV),
            P(KV),
            P(KV),
            P(KV),
            P(KV),
            P(KV, None),
            P("tp", None, KV, None, None),
            P("tp", None, KV),
            P("tp", None, KV),
            P("tp"),
        ),
        out_specs=(
            P("tp", KV),
            P("tp", None, KV, None, None),
            P("tp", None, KV),
            P("tp", None, KV),
        ),
        check_vma=False,
    )
```

```python
import jax
import jax.numpy as jnp
from jax import lax
from jax.experimental import pallas as pl
from jax.experimental.pallas import tpu as pltpu
from jax.sharding import Mesh
from jax.sharding import PartitionSpec as P


D = 4096
PROPS = 4
INNER = 8192
KV = ("z", "yh", "yl", "c")
NEAR = ("yl", "c", "tp")
EPSILON = 1e-05
TP = 4
NEAR_KV = 4
KV_SIZE = 128
SEQS = 8
HALF = 4
TOKENS = 32
HEAD = 64
STATE = 128
LINES = 6
TILE = (8, 128)
FAR_ORDER = (11, 0, 1, 2, 3, 4, 5, 6, 7, 8, 9, 10, 12, 13, 14, 15)
SMALL = 64

F32 = jnp.float32
BF16 = jnp.bfloat16


def rounded(value):
    return value.astype(BF16).astype(F32)


def lanes_of(shape):
    return lax.broadcasted_iota(jnp.int32, shape, len(shape) - 1)


def rows_of(shape):
    return lax.broadcasted_iota(jnp.int32, shape, len(shape) - 2)


def dot_nt(a, b):
    return lax.dot_general(a, b, (((1,), (1,)), ((), ())), preferred_element_type=F32)


def silu(v):
    return v / (1.0 + jnp.exp(-v))


def softplus(v):
    return jnp.maximum(v, 0.0) + jnp.log1p(jnp.exp(-jnp.abs(v)))


def tiles(value):
    return [value[8 * i : 8 * i + 8] for i in range(value.shape[0] // 8)]


def swapped(tile):
    return pltpu.roll(tile, HEAD, 1)


def turned_half(tile):
    return pltpu.roll(tile, HALF, 0)


def widened(tile):
    return jnp.concatenate([tile, jnp.zeros(tile.shape, tile.dtype)], axis=1)


def kept_rows(history, accepted):
    line = jnp.broadcast_to(accepted[...].astype(F32)[None, :], (SEQS, SEQS))
    own = lanes_of((SEQS, SEQS)) == rows_of((SEQS, SEQS))
    column = jnp.sum(jnp.where(own, line, 0.0), axis=1, keepdims=True)
    whole = [history[i].astype(F32) for i in range(7)]
    kept = []
    for m in range(3):
        row = whole[m]
        for a in range(1, PROPS + 1):
            row = jnp.where(column == float(a), whole[m + a], row)
        kept.append(row)
    return kept


def convolved(window, taps):
    results = []
    for t in range(PROPS):
        running = window[t] * taps[0]
        for j in range(1, 4):
            running = running + window[t + j] * taps[j]
        results.append(silu(running))
    return results


def three_terms(value, shape):
    value = jnp.broadcast_to(value, shape)
    high = rounded(value)
    middle = rounded(value - high)
    lanes = lanes_of(shape)
    low = value - high - middle
    return jnp.where(lanes == HEAD, high, jnp.where(lanes == HEAD + 1, middle, jnp.where(lanes == HEAD + 2, low, 0.0)))


def project_body(
    accepted_far,
    saved,
    hidden_far,
    x_weight_far,
    z_weight_far,
    bc_weight_far,
    gain_far,
    dt_weight_far,
    bc_history_far,
    bc_kernel_far,
    message,
    first_state,
    chosen,
    accepted,
    hidden,
    x_weight,
    z_weight,
    bc_weight,
    gain,
    dt_weight,
    bc_history,
    bc_kernel,
    first,
    second,
    blocks,
    coming,
    reading,
    leaving,
):
    sources = [
        accepted_far,
        hidden_far,
        x_weight_far,
        z_weight_far,
        bc_weight_far,
        gain_far,
        dt_weight_far,
        bc_history_far,
        bc_kernel_far,
        accepted_far,
    ]
    targets = [chosen, hidden, x_weight, z_weight, bc_weight, gain, dt_weight, bc_history, bc_kernel, accepted]
    inputs = [pltpu.make_async_copy(a, b, coming.at[i]) for i, (a, b) in enumerate(zip(sources, targets))]
    for copy in inputs:
        copy.start()
    inputs[0].wait()
    reads = [
        pltpu.make_async_copy(saved.at[s, chosen[s], 0], first_state.at[s], reading.at[s]) for s in range(SEQS)
    ]
    for copy in reads:
        copy.start()
    for copy in inputs[1:]:
        copy.wait()
    wide = hidden[...].astype(F32)
    scaled = (wide * gain[...].astype(F32)[None, :]).astype(BF16)
    squares = jnp.sum(wide * wide, axis=1, keepdims=True)
    dt_rows = jnp.broadcast_to(dt_weight[...], (HEAD, dt_weight.shape[1]))
    first[...] = dot_nt(scaled, jnp.concatenate([x_weight[...], z_weight[...]], axis=0))
    last = dot_nt(scaled, jnp.concatenate([bc_weight[...], dt_rows], axis=0))
    second[...] = last
    turned = jnp.transpose(jnp.where(lanes_of((128, 128)) == HEAD + 1, squares, last))
    dt_line = jnp.broadcast_to(turned[HEAD : HEAD + 1], TILE)
    square_line = jnp.broadcast_to(turned[HEAD + 1 : HEAD + 2], TILE)
    square_high = rounded(square_line)
    rows = rows_of(TILE)
    upper = lanes_of(TILE) >= HEAD
    lines = jnp.where(rows == 4, dt_line, jnp.where(rows == 5, square_high, square_line - square_high))
    empty = jnp.zeros((SEQS, HEAD), F32)
    extra = [jnp.concatenate([empty, row], axis=1) for row in kept_rows(bc_history, accepted)]
    taps = jnp.concatenate([bc_kernel[...].astype(F32), jnp.zeros((4, HEAD), F32)], axis=0)
    taps = jnp.concatenate([empty, taps], axis=1)
    copies = []
    for j in range(TP):
        top = [first[pl.ds(TOKENS * j + t, SEQS, stride=PROPS), :] for t in range(PROPS)]
        low = [second[pl.ds(TOKENS * j + t, SEQS, stride=PROPS), :] for t in range(PROPS)]
        ending = jnp.where(rows < 4, taps, pltpu.roll(lines, (64 - 32 * j) % 128, 1))
        low = [jnp.where(upper, e, v) for e, v in zip([*extra, ending], low)]
        blocks[j] = jnp.concatenate(top + low, axis=0).astype(BF16)
        for g in range(NEAR_KV):
            copies.append(pltpu.make_async_copy(blocks.at[j], message.at[g * TP + j], leaving.at[g * TP + j]))
            copies[-1].start()
    for copy in reads + copies:
        copy.wait()


def pack_body(
    dt_bias,
    decay_log,
    skip_scale,
    accepted,
    first_state,
    weight,
    x_history,
    x_kernel,
    output_gain,
    kept_pack,
    sent,
):
    core = lax.axis_index("c")
    rows = rows_of(TILE)
    terms = [three_terms(number[0], TILE) for number in (dt_bias, decay_log, skip_scale)]
    gain_row = jnp.concatenate([jnp.zeros((1, HEAD), F32), output_gain[...].astype(F32)], axis=1)
    kernel = x_kernel[...].astype(F32)
    small = [widened(row) for row in kept_rows(x_history, accepted)]
    small = [jnp.where(core == 1, turned_half(tile), tile) for tile in small]
    small += [jnp.broadcast_to(widened(kernel[j : j + 1]), TILE) for j in range(4)]
    small = [small[0] + gain_row] + [a + b for a, b in zip(small[1:4], terms)] + small[4:]
    small.append(jnp.zeros(TILE, F32))
    kept_pack[0:SMALL, :] = jnp.concatenate([jnp.where(rows < HALF, tile, 0.0) for tile in small], axis=0).astype(BF16)
    for i in range(HALF):
        own = HALF * core + i
        kept_pack[SMALL + HEAD * i : SMALL + HEAD * (i + 1), :] = first_state[own].astype(BF16)
    sent[0:HEAD, :] = weight[...]
    small = [jnp.where(rows < HALF, 0.0, tile) for tile in small]
    blocks = [jnp.concatenate(small[2 * i : 2 * i + 2], axis=0) for i in range(SMALL // 16)]
    for i in range(HALF):
        other = HALF - HALF * core + i
        state = first_state[other]
        blocks += [state[16 * k : 16 * k + 16] for k in range(HEAD // 16)]
    blocks += [jnp.zeros((16, 128), F32)] * (weight.shape[1] // 128 - len(blocks))
    for i, block in enumerate(blocks):
        sent[HEAD : HEAD + 16, 128 * i : 128 * i + 128] = block.astype(BF16)


def summed_over_tp(arrived, place, start):
    total = arrived[place * TP, start : 2 * TOKENS, :].astype(F32)
    for k in range(1, TP):
        total = total + arrived[place * TP + k, start : 2 * TOKENS, :].astype(F32)
    return tiles(total)


def scale_line(ending):
    return lax.rsqrt((ending[5:6] + ending[6:7]) / D + EPSILON)


def mix_body(arrived, kept_pack, got, weight, message, columns, block_rows, leaving):
    core = lax.axis_index("c")
    pair = lax.axis_index("yl") * 2
    mine = lax.axis_index("tp")
    lanes = lanes_of(TILE)
    rows = rows_of(TILE)
    lower = lanes < HEAD
    first_rows = rows < HALF
    second_core = core == 1

    def halves(own, other):
        own = jnp.where(second_core, turned_half(own), own)
        other = jnp.where(second_core, other, turned_half(other))
        return jnp.where(rows_of(own.shape) < HALF, own, other)

    here = pair + 1 - core
    own = summed_over_tp(arrived, here, 0)
    other = summed_over_tp(arrived, pair + core, 0)
    got_small = [got[HEAD : HEAD + 16, 128 * i : 128 * i + 128] for i in range(SMALL // 16)]
    small = tiles(kept_pack[0:SMALL, :].astype(F32) + jnp.concatenate(got_small, axis=0).astype(F32))
    gain = swapped(small[0])
    bias, decay, skip = [
        tile[:, HEAD : HEAD + 1] + tile[:, HEAD + 1 : HEAD + 2] + tile[:, HEAD + 2 : HEAD + 3] for tile in small[1:4]
    ]
    ending = own[7]
    lined = jnp.where(rows == 0, jnp.broadcast_to(scale_line(ending), TILE), ending)
    lined = jnp.where(rows == 1, jnp.broadcast_to(other[7][4:5], TILE), lined)
    columns[...] = jnp.transpose(lined)[HEAD : HEAD + TOKENS]
    rate = jnp.exp(decay)
    scale, step, cumulated = [], [], []
    total = jnp.zeros((SEQS, 1), F32)
    for t in range(PROPS):
        column = columns[pl.ds(t, SEQS, stride=PROPS), :]
        column = halves(column, column)
        scale.append(column[:, 0:1])
        raw = jnp.where(rows_of((SEQS, 1)) < HALF, column[:, 4:5], column[:, 1:2])
        step.append(softplus(rounded(scale[t] * raw) + bias))
        total = total - rate * step[t]
        cumulated.append(total)
    fresh = [rounded(scale[t] * halves(own[t], other[t])) for t in range(PROPS)]
    sums, extras = [], []
    for g in range(NEAR_KV):
        sums.append(summed_over_tp(arrived, g ^ 1, TOKENS))
        extras.append(tiles(arrived[(g ^ 1) * TP + mine, TOKENS : 2 * TOKENS, :].astype(F32)))

    def terms(left, right):
        window = [jnp.where(lower, swapped(extras[left][m]), extras[right][m]) for m in range(4)]
        new = [jnp.where(lower, sums[left][t], swapped(sums[right][t])) for t in range(PROPS)]
        taps = [window[3][j : j + 1] for j in range(4)]
        window = [halves(tile, tile) for tile in window[:3]]
        return convolved(window + [rounded(scale[t] * halves(new[t], new[t])) for t in range(PROPS)], taps)

    b_terms = terms(0, 1)
    c_terms = terms(2, 3)
    x_conv = convolved(small[0:3] + fresh, small[3:7])
    spans = range(SMALL // 16, (SMALL + HALF * HEAD) // 16)
    got_states = [got[HEAD : HEAD + 16, 128 * i : 128 * i + 128] for i in spans]
    states = jnp.concatenate([kept_pack[SMALL:, :], *got_states], axis=0)
    read = dot_nt(jnp.concatenate(c_terms, axis=0).astype(BF16), states)
    scaled = []
    squares = jnp.zeros(TILE, F32)
    quarter = lanes // TOKENS
    for t in range(PROPS):
        picked = jnp.zeros(TILE, F32)
        for k in range(SEQS // 2):
            picked = jnp.where(rows // 2 == k, read[8 * t : 8 * t + 8, 128 * k : 128 * k + 128], picked)
        picked = jnp.where(rows % 2 == 0, picked, swapped(picked))
        output = jnp.exp(cumulated[t]) * picked
        for r in range(t + 1):
            product = jnp.sum(c_terms[t] * b_terms[r], axis=1, keepdims=True)
            output = output + (jnp.exp(cumulated[t] - cumulated[r]) * step[r] * product) * x_conv[r]
        output = output + skip * x_conv[t]
        gated = output * silu(swapped(fresh[t]))
        both = jnp.where(lower, gated, swapped(turned_half(gated)))
        squares = jnp.where(quarter == t, jnp.sum(both * both, axis=1, keepdims=True), squares)
        gains = jnp.where(lower, gain, swapped(turned_half(gain)))
        scaled.append(both * gains)
    turns = []
    for d in range(4):
        turns += [row if d == 0 else pltpu.roll(row, 8 - 2 * d, 0) for row in scaled]
    turns = jnp.concatenate(turns, axis=0).astype(BF16)
    spot = jnp.where(first_rows & (lanes % TOKENS == rows), squares, 0.0)
    square_line = jnp.sum(spot, axis=0, keepdims=True)
    high = rounded(square_line)
    lines = jnp.where(rows % 2 == 0, high, square_line - high)
    copies = []
    for i, eight in enumerate(FAR_ORDER):
        cut = slice(256 * eight, 256 * (eight + 1))
        both_weights = jnp.concatenate([weight[:, cut], got[0:HEAD, cut]], axis=0)
        product = jnp.dot(turns, both_weights, preferred_element_type=F32)
        pieces = []
        for half in range(2):
            block = product[:, 128 * half : 128 * (half + 1)]
            spots = []
            for d in range(4):
                spot = None
                for t in range(PROPS):
                    piece = block[32 * d + 8 * t : 32 * d + 8 * t + 8]
                    piece = piece if t == d ^ 1 else pltpu.roll(piece, (32 * (t - (d ^ 1))) % 128, 1)
                    spot = piece if t == 0 else jnp.where(quarter == t, piece, spot)
                spots.append(spot)
            pieces += [
                jnp.where(rows < 4, spots[0], jnp.where(rows < 6, lines, spots[1])),
                jnp.where(rows < 2, spots[1], jnp.where(rows < 4, lines, spots[2])),
                jnp.where((rows >= 2) & (rows < 6), spots[3], lines),
            ]
        block_rows[48 * i : 48 * (i + 1), :] = jnp.concatenate(pieces, axis=0).astype(BF16)
        if i % 4 == 3:
            part = pl.ds(48 * (i - 3), 192)
            copies.append(pltpu.make_async_copy(block_rows.at[part], message.at[part], leaving.at[i // 4]))
            copies[-1].start()
    for copy in copies:
        copy.wait()


def state_body(
    dt_bias,
    decay_log,
    accepted,
    arrived,
    first_state,
    x_kernel,
    x_history,
    new_states,
    x_window,
    bc_window,
    columns,
):
    place = lax.axis_index("yl") * 2 + 1 - lax.axis_index("c")
    mine = lax.axis_index("tp")
    lanes = lanes_of(TILE)
    lower = lanes < HEAD
    own = summed_over_tp(arrived, place, 0)
    ending = own[7]
    lined = jnp.where(rows_of(TILE) == 0, jnp.broadcast_to(scale_line(ending), TILE), ending)
    columns[...] = jnp.transpose(lined)[HEAD : HEAD + TOKENS]
    bias = dt_bias[0]
    rate = jnp.exp(jnp.full((SEQS, 1), decay_log[0], F32))
    scale, step = [], []
    for t in range(PROPS):
        column = columns[pl.ds(t, SEQS, stride=PROPS), :]
        scale.append(column[:, 0:1])
        step.append(softplus(rounded(scale[t] * column[:, 4:5]) + bias))
    fresh = [rounded(scale[t] * own[t]) for t in range(PROPS)]
    sums = [summed_over_tp(arrived, g ^ 1, TOKENS) for g in range(2)]
    extras = [tiles(arrived[(g ^ 1) * TP + mine, TOKENS : 2 * TOKENS, :].astype(F32)) for g in range(2)]
    window = [jnp.where(lower, swapped(extras[0][m]), extras[1][m]) for m in range(4)]
    new = [rounded(scale[t] * jnp.where(lower, sums[0][t], swapped(sums[1][t]))) for t in range(PROPS)]
    b_terms = convolved(window[:3] + new, [window[3][j : j + 1] for j in range(4)])
    kept = kept_rows(x_history, accepted)
    kernel = widened(x_kernel[...].astype(F32))
    x_conv = convolved([widened(row) for row in kept] + fresh, [kernel[j : j + 1] for j in range(4)])
    inputs = [x_conv[t] * step[t] for t in range(PROPS)]
    turned = jnp.transpose(jnp.concatenate(inputs + [jnp.zeros((128 - TOKENS, 128), F32)], axis=0))[:HEAD]
    decay = [jnp.broadcast_to(jnp.exp(-rate * step[t]), TILE) for t in range(PROPS)]
    for s in range(SEQS):
        state = first_state[s]
        new_states[s, 0, 0] = state
        for t in range(PROPS):
            at = 8 * t + s
            state = state * decay[t][s : s + 1, :] + turned[:, at : at + 1] * b_terms[t][s : s + 1, :]
            new_states[s, t + 1, 0] = state
    own_extra = tiles(arrived[place * TP + mine, TOKENS : 2 * TOKENS, :].astype(F32))
    for m in range(3):
        x_window[m] = kept[m].astype(BF16)
        bc_window[m] = swapped(own_extra[m])[:, :HEAD].astype(BF16)
    for t in range(PROPS):
        x_window[3 + t] = fresh[t][:, :HEAD].astype(BF16)
        bc_window[3 + t] = (scale[t] * own[4 + t])[:, :HEAD].astype(BF16)


def finish_body(arrived, mixed, total, placed):
    step = 8 * LINES
    running = arrived[0:step, :].astype(F32)
    for i in range(1, arrived.shape[0] // step):
        running = running + arrived[step * i : step * (i + 1), :].astype(F32)
    total[...] = running
    sums = []
    for c in range(2):
        start = LINES * (1 - c)
        part = total[start : start + LINES, :]
        for i in range(1, 4):
            part = part + total[2 * LINES * i + start : 2 * LINES * i + start + LINES, :]
        sums.append(part)
    summed = jnp.concatenate([part[:HALF] for part in sums], axis=0)
    means = [jnp.broadcast_to((part[4:5] + part[5:6]) / INNER, (HALF, 128)) for part in sums]
    mean = jnp.concatenate(means, axis=0)
    lanes = lanes_of(TILE)
    rows = rows_of(TILE)
    for t in range(PROPS):
        own = jnp.sum(jnp.where(lanes == TOKENS * t + rows % HALF, mean, 0.0), axis=1, keepdims=True)
        moved = summed if t == 0 else pltpu.roll(summed, 128 - TOKENS * t, 1)
        placed[pl.ds(t, SEQS, stride=PROPS), :] = lax.rsqrt(own + EPSILON) * moved
    mixed[...] = placed[...][:, :TOKENS].astype(BF16)


def smem():
    return pl.BlockSpec(memory_space=pltpu.SMEM)


def vmem():
    return pl.BlockSpec(memory_space=pltpu.VMEM)


def far_memory():
    return pl.BlockSpec(memory_space=pltpu.HBM)


def near_memory(value):
    return pltpu.with_memory_space_constraint(value, pltpu.VMEM)


def local(
    hidden,
    input_gain,
    x_weight,
    z_weight,
    bc_weight,
    dt_weight,
    x_kernel,
    bc_kernel,
    dt_bias,
    decay_log,
    skip_scale,
    output_gain,
    output_weight,
    saved_states,
    x_history,
    bc_history,
    accepted,
):
    shape = jax.ShapeDtypeStruct
    held = pltpu.VMEM
    lines = KV_SIZE * LINES
    x_rows = jnp.transpose(x_history, (1, 0, 2))
    bc_rows = jnp.transpose(bc_history, (1, 0, 2))
    pack_rows = SMALL + HALF * HEAD
    near, first_state = pl.pallas_call(
        project_body,
        out_shape=(shape((TP * NEAR_KV, 2 * TOKENS, 128), BF16), held((SEQS, HEAD, STATE), F32)),
        in_specs=[far_memory()] * 10,
        out_specs=(far_memory(), vmem()),
        scratch_shapes=[
            pltpu.SMEM(accepted.shape, jnp.int32),
            pltpu.VMEM(accepted.shape, jnp.int32),
            pltpu.VMEM(hidden.shape, BF16),
            pltpu.VMEM(x_weight.T.shape, BF16),
            pltpu.VMEM(z_weight.T.shape, BF16),
            pltpu.VMEM(bc_weight.T.shape, BF16),
            pltpu.VMEM(input_gain.shape, BF16),
            pltpu.VMEM(dt_weight.T.shape, BF16),
            pltpu.VMEM(bc_rows.shape, BF16),
            pltpu.VMEM(bc_kernel.shape, BF16),
            pltpu.VMEM((128, 128), F32),
            pltpu.VMEM((128, 128), F32),
            pltpu.VMEM((TP, 2 * TOKENS, 128), BF16),
            pltpu.SemaphoreType.DMA((10,)),
            pltpu.SemaphoreType.DMA((SEQS,)),
            pltpu.SemaphoreType.DMA((TP * NEAR_KV,)),
        ],
    )(accepted, saved_states, hidden, x_weight.T, z_weight.T, bc_weight.T, input_gain, dt_weight.T, bc_rows, bc_kernel)
    first_state = near_memory(first_state)
    output_weight = near_memory(output_weight)
    order = [[(g ^ 1) * TP + k for g in range(NEAR_KV) for k in range(TP)]]
    arrived = near_memory(lax.all_to_all(near, NEAR, 0, 0, tiled=True, axis_index_groups=order))
    kept_pack, sent = pl.pallas_call(
        pack_body,
        out_shape=(held((pack_rows, 128), BF16), held((HEAD + 16, output_weight.shape[1]), BF16)),
        in_specs=[smem()] * 3 + [vmem()] * 6,
        out_specs=(vmem(),) * 2,
        cost_estimate=pl.CostEstimate(flops=4_000_000, bytes_accessed=3_000_000, transcendentals=0),
    )(
        dt_bias,
        decay_log,
        skip_scale,
        near_memory(accepted),
        first_state,
        output_weight,
        near_memory(x_rows),
        near_memory(x_kernel),
        near_memory(output_gain.reshape(1, HEAD)),
    )
    got = lax.ppermute(sent, "c", [(0, 1), (1, 0)])
    far = pl.pallas_call(
        mix_body,
        out_shape=shape((lines, 128), BF16),
        in_specs=[vmem()] * 4,
        out_specs=far_memory(),
        scratch_shapes=[pltpu.VMEM((TOKENS, 8), F32), pltpu.VMEM((lines, 128), BF16), pltpu.SemaphoreType.DMA((4,))],
    )(arrived, near_memory(kept_pack), near_memory(got), output_weight)
    order = [[8 * eight + (i ^ 1) for eight in FAR_ORDER for i in range(8)]]
    far = far.reshape(KV_SIZE, LINES // 2, 2, 128)
    landed = lax.all_to_all(far, KV, 0, 0, tiled=True, axis_index_groups=order)
    landed = near_memory(landed.reshape(lines, 128))
    new_states, x_window, bc_window = pl.pallas_call(
        state_body,
        out_shape=(
            shape((SEQS, PROPS + 1, 1, HEAD, STATE), F32),
            shape((7, SEQS, HEAD), BF16),
            shape((7, SEQS, HEAD), BF16),
        ),
        in_specs=[smem()] * 2 + [vmem()] * 5,
        out_specs=(vmem(),) * 3,
        scratch_shapes=[pltpu.VMEM((TOKENS, 8), F32)],
        cost_estimate=pl.CostEstimate(flops=4_000_000, bytes_accessed=3_000_000, transcendentals=0),
    )(
        dt_bias,
        decay_log,
        accepted,
        arrived,
        first_state,
        x_kernel,
        x_rows,
    )
    mixed = pl.pallas_call(
        finish_body,
        out_shape=shape((TOKENS, TOKENS), BF16),
        in_specs=[vmem()],
        out_specs=vmem(),
        scratch_shapes=[pltpu.VMEM((8 * LINES, 128), F32), pltpu.VMEM((TOKENS, 128), F32)],
    )(landed)
    return (mixed, new_states, jnp.transpose(x_window, (1, 0, 2)), jnp.transpose(bc_window, (1, 0, 2)))


def solution(mesh):
    split = Mesh(mesh.devices.reshape(8, 4, 2, 2, mesh.shape["tp"]), ("z", "yh", "yl", "c", "tp"))
    return jax.shard_map(
        local,
        mesh=split,
        in_specs=(
            P(None, "tp"),
            P("tp"),
            P("tp", KV),
            P("tp", KV),
            P("tp", KV),
            P("tp", KV),
            P(None, KV),
            P(None, KV),
            P(KV),
            P(KV),
            P(KV),
            P(KV),
            P(KV, None),
            P("tp", None, KV, None, None),
            P("tp", None, KV),
            P("tp", None, KV),
            P("tp"),
        ),
        out_specs=(
            P("tp", KV),
            P("tp", None, KV, None, None),
            P("tp", None, KV),
            P("tp", None, KV),
        ),
        check_vma=False,
    )
```

```python
import jax
import jax.numpy as jnp
from jax import lax
from jax.experimental import pallas as pl
from jax.experimental.pallas import tpu as pltpu
from jax.sharding import Mesh
from jax.sharding import PartitionSpec as P


D = 4096
PROPS = 4
INNER = 8192
KV = ("z", "yh", "yl", "c")
NEAR = ("yl", "c", "tp")
EPSILON = 1e-05
TP = 4
NEAR_KV = 4
KV_SIZE = 128
SEQS = 8
HALF = 4
TOKENS = 32
HEAD = 64
STATE = 128
LINES = 6
TILE = (8, 128)
FAR_ORDER = (11, 0, 1, 2, 3, 4, 5, 6, 7, 8, 9, 10, 12, 13, 14, 15)
SMALL = 64

F32 = jnp.float32
BF16 = jnp.bfloat16


def rounded(value):
    return value.astype(BF16).astype(F32)


def lanes_of(shape):
    return lax.broadcasted_iota(jnp.int32, shape, len(shape) - 1)


def rows_of(shape):
    return lax.broadcasted_iota(jnp.int32, shape, len(shape) - 2)


def dot_nt(a, b):
    return lax.dot_general(a, b, (((1,), (1,)), ((), ())), preferred_element_type=F32)


def silu(v):
    return v / (1.0 + jnp.exp(-v))


def softplus(v):
    return jnp.maximum(v, 0.0) + jnp.log1p(jnp.exp(-jnp.abs(v)))


def tiles(value):
    return [value[8 * i : 8 * i + 8] for i in range(value.shape[0] // 8)]


def swapped(tile):
    return pltpu.roll(tile, HEAD, 1)


def turned_half(tile):
    return pltpu.roll(tile, HALF, 0)


def widened(tile):
    return jnp.concatenate([tile, jnp.zeros(tile.shape, tile.dtype)], axis=1)


def kept_rows(history, accepted):
    line = jnp.broadcast_to(accepted[...].astype(F32)[None, :], (SEQS, SEQS))
    own = lanes_of((SEQS, SEQS)) == rows_of((SEQS, SEQS))
    column = jnp.sum(jnp.where(own, line, 0.0), axis=1, keepdims=True)
    whole = [history[i].astype(F32) for i in range(7)]
    kept = []
    for m in range(3):
        row = whole[m]
        for a in range(1, PROPS + 1):
            row = jnp.where(column == float(a), whole[m + a], row)
        kept.append(row)
    return kept


def convolved(window, taps):
    results = []
    for t in range(PROPS):
        running = window[t] * taps[0]
        for j in range(1, 4):
            running = running + window[t + j] * taps[j]
        results.append(silu(running))
    return results


def three_terms(value, shape):
    value = jnp.broadcast_to(value, shape)
    high = rounded(value)
    middle = rounded(value - high)
    lanes = lanes_of(shape)
    low = value - high - middle
    return jnp.where(lanes == HEAD, high, jnp.where(lanes == HEAD + 1, middle, jnp.where(lanes == HEAD + 2, low, 0.0)))


def project_body(
    accepted_far,
    saved,
    hidden_far,
    x_weight_far,
    z_weight_far,
    bc_weight_far,
    gain_far,
    dt_weight_far,
    bc_history_far,
    bc_kernel_far,
    weight_far,
    message,
    first_state,
    weight,
    chosen,
    accepted,
    hidden,
    x_weight,
    z_weight,
    bc_weight,
    gain,
    dt_weight,
    bc_history,
    bc_kernel,
    first,
    second,
    blocks,
    coming,
    reading,
    leaving,
):
    sources = [
        accepted_far,
        hidden_far,
        x_weight_far,
        z_weight_far,
        bc_weight_far,
        gain_far,
        dt_weight_far,
        bc_history_far,
        bc_kernel_far,
        accepted_far,
    ]
    targets = [chosen, hidden, x_weight, z_weight, bc_weight, gain, dt_weight, bc_history, bc_kernel, accepted]
    inputs = [pltpu.make_async_copy(a, b, coming.at[i]) for i, (a, b) in enumerate(zip(sources, targets))]
    for copy in inputs:
        copy.start()
    weight_copy = pltpu.make_async_copy(weight_far, weight, reading.at[SEQS])
    inputs[0].wait()
    reads = [
        pltpu.make_async_copy(saved.at[s, chosen[s], 0], first_state.at[s], reading.at[s]) for s in range(SEQS)
    ]
    reads.append(weight_copy)
    for copy in reads:
        copy.start()
    for copy in inputs[1:]:
        copy.wait()
    wide = hidden[...].astype(F32)
    scaled = (wide * gain[...].astype(F32)[None, :]).astype(BF16)
    squares = jnp.sum(wide * wide, axis=1, keepdims=True)
    dt_rows = jnp.broadcast_to(dt_weight[...], (HEAD, dt_weight.shape[1]))
    first[...] = dot_nt(scaled, jnp.concatenate([x_weight[...], z_weight[...]], axis=0))
    last = dot_nt(scaled, jnp.concatenate([bc_weight[...], dt_rows], axis=0))
    second[...] = last
    turned = jnp.transpose(jnp.where(lanes_of((128, 128)) == HEAD + 1, squares, last))
    dt_line = jnp.broadcast_to(turned[HEAD : HEAD + 1], TILE)
    square_line = jnp.broadcast_to(turned[HEAD + 1 : HEAD + 2], TILE)
    square_high = rounded(square_line)
    rows = rows_of(TILE)
    upper = lanes_of(TILE) >= HEAD
    lines = jnp.where(rows == 4, dt_line, jnp.where(rows == 5, square_high, square_line - square_high))
    empty = jnp.zeros((SEQS, HEAD), F32)
    extra = [jnp.concatenate([empty, row], axis=1) for row in kept_rows(bc_history, accepted)]
    taps = jnp.concatenate([bc_kernel[...].astype(F32), jnp.zeros((4, HEAD), F32)], axis=0)
    taps = jnp.concatenate([empty, taps], axis=1)
    copies = []
    for j in range(TP):
        top = [first[pl.ds(TOKENS * j + t, SEQS, stride=PROPS), :] for t in range(PROPS)]
        low = [second[pl.ds(TOKENS * j + t, SEQS, stride=PROPS), :] for t in range(PROPS)]
        ending = jnp.where(rows < 4, taps, pltpu.roll(lines, (64 - 32 * j) % 128, 1))
        low = [jnp.where(upper, e, v) for e, v in zip([*extra, ending], low)]
        blocks[j] = jnp.concatenate(top + low, axis=0).astype(BF16)
        for g in range(NEAR_KV):
            copies.append(pltpu.make_async_copy(blocks.at[j], message.at[g * TP + j], leaving.at[g * TP + j]))
            copies[-1].start()
    for copy in reads + copies:
        copy.wait()


def pack_body(
    dt_bias,
    decay_log,
    skip_scale,
    accepted,
    first_state,
    weight,
    x_history,
    x_kernel,
    output_gain,
    kept_pack,
    sent,
):
    core = lax.axis_index("c")
    rows = rows_of(TILE)
    terms = [three_terms(number[0], TILE) for number in (dt_bias, decay_log, skip_scale)]
    gain_row = jnp.concatenate([jnp.zeros((1, HEAD), F32), output_gain[...].astype(F32)], axis=1)
    kernel = x_kernel[...].astype(F32)
    small = [widened(row) for row in kept_rows(x_history, accepted)]
    small = [jnp.where(core == 1, turned_half(tile), tile) for tile in small]
    small += [jnp.broadcast_to(widened(kernel[j : j + 1]), TILE) for j in range(4)]
    small = [small[0] + gain_row] + [a + b for a, b in zip(small[1:4], terms)] + small[4:]
    small.append(jnp.zeros(TILE, F32))
    kept_pack[0:SMALL, :] = jnp.concatenate([jnp.where(rows < HALF, tile, 0.0) for tile in small], axis=0).astype(BF16)
    for i in range(HALF):
        own = HALF * core + i
        kept_pack[SMALL + HEAD * i : SMALL + HEAD * (i + 1), :] = first_state[own].astype(BF16)
    sent[0:HEAD, :] = weight[...]
    small = [jnp.where(rows < HALF, 0.0, tile) for tile in small]
    blocks = [jnp.concatenate(small[2 * i : 2 * i + 2], axis=0) for i in range(SMALL // 16)]
    for i in range(HALF):
        other = HALF - HALF * core + i
        state = first_state[other]
        blocks += [state[16 * k : 16 * k + 16] for k in range(HEAD // 16)]
    blocks += [jnp.zeros((16, 128), F32)] * (weight.shape[1] // 128 - len(blocks))
    for i, block in enumerate(blocks):
        sent[HEAD : HEAD + 16, 128 * i : 128 * i + 128] = block.astype(BF16)


def summed_over_tp(arrived, place, start):
    total = arrived[place * TP, start : 2 * TOKENS, :].astype(F32)
    for k in range(1, TP):
        total = total + arrived[place * TP + k, start : 2 * TOKENS, :].astype(F32)
    return tiles(total)


def scale_line(ending):
    return lax.rsqrt((ending[5:6] + ending[6:7]) / D + EPSILON)


def mix_body(arrived, kept_pack, got, weight, message, columns, block_rows, leaving):
    core = lax.axis_index("c")
    pair = lax.axis_index("yl") * 2
    mine = lax.axis_index("tp")
    lanes = lanes_of(TILE)
    rows = rows_of(TILE)
    lower = lanes < HEAD
    first_rows = rows < HALF
    second_core = core == 1

    def halves(own, other):
        own = jnp.where(second_core, turned_half(own), own)
        other = jnp.where(second_core, other, turned_half(other))
        return jnp.where(rows_of(own.shape) < HALF, own, other)

    here = pair + 1 - core
    own = summed_over_tp(arrived, here, 0)
    other = summed_over_tp(arrived, pair + core, 0)
    got_small = [got[HEAD : HEAD + 16, 128 * i : 128 * i + 128] for i in range(SMALL // 16)]
    small = tiles(kept_pack[0:SMALL, :].astype(F32) + jnp.concatenate(got_small, axis=0).astype(F32))
    gain = swapped(small[0])
    bias, decay, skip = [
        tile[:, HEAD : HEAD + 1] + tile[:, HEAD + 1 : HEAD + 2] + tile[:, HEAD + 2 : HEAD + 3] for tile in small[1:4]
    ]
    ending = own[7]
    lined = jnp.where(rows == 0, jnp.broadcast_to(scale_line(ending), TILE), ending)
    lined = jnp.where(rows == 1, jnp.broadcast_to(other[7][4:5], TILE), lined)
    columns[...] = jnp.transpose(lined)[HEAD : HEAD + TOKENS]
    rate = jnp.exp(decay)
    scale, step, cumulated = [], [], []
    total = jnp.zeros((SEQS, 1), F32)
    for t in range(PROPS):
        column = columns[pl.ds(t, SEQS, stride=PROPS), :]
        column = halves(column, column)
        scale.append(column[:, 0:1])
        raw = jnp.where(rows_of((SEQS, 1)) < HALF, column[:, 4:5], column[:, 1:2])
        step.append(softplus(rounded(scale[t] * raw) + bias))
        total = total - rate * step[t]
        cumulated.append(total)
    fresh = [rounded(scale[t] * halves(own[t], other[t])) for t in range(PROPS)]
    sums, extras = [], []
    for g in range(NEAR_KV):
        sums.append(summed_over_tp(arrived, g ^ 1, TOKENS))
        extras.append(tiles(arrived[(g ^ 1) * TP + mine, TOKENS : 2 * TOKENS, :].astype(F32)))

    def terms(left, right):
        window = [jnp.where(lower, swapped(extras[left][m]), extras[right][m]) for m in range(4)]
        new = [jnp.where(lower, sums[left][t], swapped(sums[right][t])) for t in range(PROPS)]
        taps = [window[3][j : j + 1] for j in range(4)]
        window = [halves(tile, tile) for tile in window[:3]]
        return convolved(window + [rounded(scale[t] * halves(new[t], new[t])) for t in range(PROPS)], taps)

    b_terms = terms(0, 1)
    c_terms = terms(2, 3)
    x_conv = convolved(small[0:3] + fresh, small[3:7])
    spans = range(SMALL // 16, (SMALL + HALF * HEAD) // 16)
    got_states = [got[HEAD : HEAD + 16, 128 * i : 128 * i + 128] for i in spans]
    states = jnp.concatenate([kept_pack[SMALL:, :], *got_states], axis=0)
    read = dot_nt(jnp.concatenate(c_terms, axis=0).astype(BF16), states)
    scaled = []
    squares = jnp.zeros(TILE, F32)
    quarter = lanes // TOKENS
    for t in range(PROPS):
        picked = jnp.zeros(TILE, F32)
        for k in range(SEQS // 2):
            picked = jnp.where(rows // 2 == k, read[8 * t : 8 * t + 8, 128 * k : 128 * k + 128], picked)
        picked = jnp.where(rows % 2 == 0, picked, swapped(picked))
        output = jnp.exp(cumulated[t]) * picked
        for r in range(t + 1):
            product = jnp.sum(c_terms[t] * b_terms[r], axis=1, keepdims=True)
            output = output + (jnp.exp(cumulated[t] - cumulated[r]) * step[r] * product) * x_conv[r]
        output = output + skip * x_conv[t]
        gated = output * silu(swapped(fresh[t]))
        both = jnp.where(lower, gated, swapped(turned_half(gated)))
        squares = jnp.where(quarter == t, jnp.sum(both * both, axis=1, keepdims=True), squares)
        gains = jnp.where(lower, gain, swapped(turned_half(gain)))
        scaled.append(both * gains)
    turns = []
    for d in range(4):
        turns += [row if d == 0 else pltpu.roll(row, 8 - 2 * d, 0) for row in scaled]
    turns = jnp.concatenate(turns, axis=0).astype(BF16)
    spot = jnp.where(first_rows & (lanes % TOKENS == rows), squares, 0.0)
    square_line = jnp.sum(spot, axis=0, keepdims=True)
    high = rounded(square_line)
    lines = jnp.where(rows % 2 == 0, high, square_line - high)
    copies = []
    for i, eight in enumerate(FAR_ORDER):
        cut = slice(256 * eight, 256 * (eight + 1))
        both_weights = jnp.concatenate([weight[:, cut], got[0:HEAD, cut]], axis=0)
        product = jnp.dot(turns, both_weights, preferred_element_type=F32)
        pieces = []
        for half in range(2):
            block = product[:, 128 * half : 128 * (half + 1)]
            spots = []
            for d in range(4):
                spot = None
                for t in range(PROPS):
                    piece = block[32 * d + 8 * t : 32 * d + 8 * t + 8]
                    piece = piece if t == d ^ 1 else pltpu.roll(piece, (32 * (t - (d ^ 1))) % 128, 1)
                    spot = piece if t == 0 else jnp.where(quarter == t, piece, spot)
                spots.append(spot)
            pieces += [
                jnp.where(rows < 4, spots[0], jnp.where(rows < 6, lines, spots[1])),
                jnp.where(rows < 2, spots[1], jnp.where(rows < 4, lines, spots[2])),
                jnp.where((rows >= 2) & (rows < 6), spots[3], lines),
            ]
        block_rows[48 * i : 48 * (i + 1), :] = jnp.concatenate(pieces, axis=0).astype(BF16)
        if i % 2 == 1:
            part = pl.ds(48 * (i - 1), 96)
            copies.append(pltpu.make_async_copy(block_rows.at[part], message.at[part], leaving.at[i // 2]))
            copies[-1].start()
    for copy in copies:
        copy.wait()


def state_body(
    dt_bias,
    decay_log,
    accepted,
    arrived,
    first_state,
    x_kernel,
    x_history,
    new_states,
    x_window,
    bc_window,
    columns,
):
    place = lax.axis_index("yl") * 2 + 1 - lax.axis_index("c")
    mine = lax.axis_index("tp")
    lanes = lanes_of(TILE)
    lower = lanes < HEAD
    own = summed_over_tp(arrived, place, 0)
    ending = own[7]
    lined = jnp.where(rows_of(TILE) == 0, jnp.broadcast_to(scale_line(ending), TILE), ending)
    columns[...] = jnp.transpose(lined)[HEAD : HEAD + TOKENS]
    bias = dt_bias[0]
    rate = jnp.exp(jnp.full((SEQS, 1), decay_log[0], F32))
    scale, step = [], []
    for t in range(PROPS):
        column = columns[pl.ds(t, SEQS, stride=PROPS), :]
        scale.append(column[:, 0:1])
        step.append(softplus(rounded(scale[t] * column[:, 4:5]) + bias))
    fresh = [rounded(scale[t] * own[t]) for t in range(PROPS)]
    sums = [summed_over_tp(arrived, g ^ 1, TOKENS) for g in range(2)]
    extras = [tiles(arrived[(g ^ 1) * TP + mine, TOKENS : 2 * TOKENS, :].astype(F32)) for g in range(2)]
    window = [jnp.where(lower, swapped(extras[0][m]), extras[1][m]) for m in range(4)]
    new = [rounded(scale[t] * jnp.where(lower, sums[0][t], swapped(sums[1][t]))) for t in range(PROPS)]
    b_terms = convolved(window[:3] + new, [window[3][j : j + 1] for j in range(4)])
    kept = kept_rows(x_history, accepted)
    kernel = widened(x_kernel[...].astype(F32))
    x_conv = convolved([widened(row) for row in kept] + fresh, [kernel[j : j + 1] for j in range(4)])
    inputs = [x_conv[t] * step[t] for t in range(PROPS)]
    turned = jnp.transpose(jnp.concatenate(inputs + [jnp.zeros((128 - TOKENS, 128), F32)], axis=0))[:HEAD]
    decay = [jnp.broadcast_to(jnp.exp(-rate * step[t]), TILE) for t in range(PROPS)]
    for s in range(SEQS):
        state = first_state[s]
        new_states[s, 0, 0] = state
        for t in range(PROPS):
            at = 8 * t + s
            state = state * decay[t][s : s + 1, :] + turned[:, at : at + 1] * b_terms[t][s : s + 1, :]
            new_states[s, t + 1, 0] = state
    own_extra = tiles(arrived[place * TP + mine, TOKENS : 2 * TOKENS, :].astype(F32))
    for m in range(3):
        x_window[m] = kept[m].astype(BF16)
        bc_window[m] = swapped(own_extra[m])[:, :HEAD].astype(BF16)
    for t in range(PROPS):
        x_window[3 + t] = fresh[t][:, :HEAD].astype(BF16)
        bc_window[3 + t] = (scale[t] * own[4 + t])[:, :HEAD].astype(BF16)


def finish_body(arrived, mixed, total, placed):
    step = 8 * LINES
    running = arrived[0:step, :].astype(F32)
    for i in range(1, arrived.shape[0] // step):
        running = running + arrived[step * i : step * (i + 1), :].astype(F32)
    total[...] = running
    sums = []
    for c in range(2):
        start = LINES * (1 - c)
        part = total[start : start + LINES, :]
        for i in range(1, 4):
            part = part + total[2 * LINES * i + start : 2 * LINES * i + start + LINES, :]
        sums.append(part)
    summed = jnp.concatenate([part[:HALF] for part in sums], axis=0)
    means = [jnp.broadcast_to((part[4:5] + part[5:6]) / INNER, (HALF, 128)) for part in sums]
    mean = jnp.concatenate(means, axis=0)
    lanes = lanes_of(TILE)
    rows = rows_of(TILE)
    for t in range(PROPS):
        own = jnp.sum(jnp.where(lanes == TOKENS * t + rows % HALF, mean, 0.0), axis=1, keepdims=True)
        moved = summed if t == 0 else pltpu.roll(summed, 128 - TOKENS * t, 1)
        placed[pl.ds(t, SEQS, stride=PROPS), :] = lax.rsqrt(own + EPSILON) * moved
    mixed[...] = placed[...][:, :TOKENS].astype(BF16)


def smem():
    return pl.BlockSpec(memory_space=pltpu.SMEM)


def vmem():
    return pl.BlockSpec(memory_space=pltpu.VMEM)


def far_memory():
    return pl.BlockSpec(memory_space=pltpu.HBM)


def near_memory(value):
    return pltpu.with_memory_space_constraint(value, pltpu.VMEM)


def local(
    hidden,
    input_gain,
    x_weight,
    z_weight,
    bc_weight,
    dt_weight,
    x_kernel,
    bc_kernel,
    dt_bias,
    decay_log,
    skip_scale,
    output_gain,
    output_weight,
    saved_states,
    x_history,
    bc_history,
    accepted,
):
    shape = jax.ShapeDtypeStruct
    held = pltpu.VMEM
    lines = KV_SIZE * LINES
    x_rows = jnp.transpose(x_history, (1, 0, 2))
    bc_rows = jnp.transpose(bc_history, (1, 0, 2))
    pack_rows = SMALL + HALF * HEAD
    near, first_state, output_weight = pl.pallas_call(
        project_body,
        out_shape=(
            shape((TP * NEAR_KV, 2 * TOKENS, 128), BF16),
            held((SEQS, HEAD, STATE), F32),
            held(output_weight.shape, BF16),
        ),
        in_specs=[far_memory()] * 11,
        out_specs=(far_memory(), vmem(), vmem()),
        scratch_shapes=[
            pltpu.SMEM(accepted.shape, jnp.int32),
            pltpu.VMEM(accepted.shape, jnp.int32),
            pltpu.VMEM(hidden.shape, BF16),
            pltpu.VMEM(x_weight.T.shape, BF16),
            pltpu.VMEM(z_weight.T.shape, BF16),
            pltpu.VMEM(bc_weight.T.shape, BF16),
            pltpu.VMEM(input_gain.shape, BF16),
            pltpu.VMEM(dt_weight.T.shape, BF16),
            pltpu.VMEM(bc_rows.shape, BF16),
            pltpu.VMEM(bc_kernel.shape, BF16),
            pltpu.VMEM((128, 128), F32),
            pltpu.VMEM((128, 128), F32),
            pltpu.VMEM((TP, 2 * TOKENS, 128), BF16),
            pltpu.SemaphoreType.DMA((10,)),
            pltpu.SemaphoreType.DMA((SEQS + 1,)),
            pltpu.SemaphoreType.DMA((TP * NEAR_KV,)),
        ],
    )(
        accepted,
        saved_states,
        hidden,
        x_weight.T,
        z_weight.T,
        bc_weight.T,
        input_gain,
        dt_weight.T,
        bc_rows,
        bc_kernel,
        output_weight,
    )
    first_state = near_memory(first_state)
    output_weight = near_memory(output_weight)
    order = [[(g ^ 1) * TP + k for g in range(NEAR_KV) for k in range(TP)]]
    arrived = near_memory(lax.all_to_all(near, NEAR, 0, 0, tiled=True, axis_index_groups=order))
    kept_pack, sent = pl.pallas_call(
        pack_body,
        out_shape=(held((pack_rows, 128), BF16), held((HEAD + 16, output_weight.shape[1]), BF16)),
        in_specs=[smem()] * 3 + [vmem()] * 6,
        out_specs=(vmem(),) * 2,
        cost_estimate=pl.CostEstimate(flops=4_000_000, bytes_accessed=3_000_000, transcendentals=0),
    )(
        dt_bias,
        decay_log,
        skip_scale,
        near_memory(accepted),
        first_state,
        output_weight,
        near_memory(x_rows),
        near_memory(x_kernel),
        near_memory(output_gain.reshape(1, HEAD)),
    )
    got = lax.ppermute(sent, "c", [(0, 1), (1, 0)])
    far = pl.pallas_call(
        mix_body,
        out_shape=shape((lines, 128), BF16),
        in_specs=[vmem()] * 4,
        out_specs=far_memory(),
        scratch_shapes=[pltpu.VMEM((TOKENS, 8), F32), pltpu.VMEM((lines, 128), BF16), pltpu.SemaphoreType.DMA((8,))],
    )(arrived, near_memory(kept_pack), near_memory(got), output_weight)
    order = [[8 * eight + (i ^ 1) for eight in FAR_ORDER for i in range(8)]]
    far = far.reshape(KV_SIZE, LINES // 2, 2, 128)
    landed = lax.all_to_all(far, KV, 0, 0, tiled=True, axis_index_groups=order)
    landed = near_memory(landed.reshape(lines, 128))
    new_states, x_window, bc_window = pl.pallas_call(
        state_body,
        out_shape=(
            shape((SEQS, PROPS + 1, 1, HEAD, STATE), F32),
            shape((7, SEQS, HEAD), BF16),
            shape((7, SEQS, HEAD), BF16),
        ),
        in_specs=[smem()] * 2 + [vmem()] * 5,
        out_specs=(vmem(),) * 3,
        scratch_shapes=[pltpu.VMEM((TOKENS, 8), F32)],
        cost_estimate=pl.CostEstimate(flops=4_000_000, bytes_accessed=3_000_000, transcendentals=0),
    )(
        dt_bias,
        decay_log,
        accepted,
        arrived,
        first_state,
        x_kernel,
        x_rows,
    )
    mixed = pl.pallas_call(
        finish_body,
        out_shape=shape((TOKENS, TOKENS), BF16),
        in_specs=[vmem()],
        out_specs=vmem(),
        scratch_shapes=[pltpu.VMEM((8 * LINES, 128), F32), pltpu.VMEM((TOKENS, 128), F32)],
    )(landed)
    return (mixed, new_states, jnp.transpose(x_window, (1, 0, 2)), jnp.transpose(bc_window, (1, 0, 2)))


def solution(mesh):
    split = Mesh(mesh.devices.reshape(8, 4, 2, 2, mesh.shape["tp"]), ("z", "yh", "yl", "c", "tp"))
    return jax.shard_map(
        local,
        mesh=split,
        in_specs=(
            P(None, "tp"),
            P("tp"),
            P("tp", KV),
            P("tp", KV),
            P("tp", KV),
            P("tp", KV),
            P(None, KV),
            P(None, KV),
            P(KV),
            P(KV),
            P(KV),
            P(KV),
            P(KV, None),
            P("tp", None, KV, None, None),
            P("tp", None, KV),
            P("tp", None, KV),
            P("tp"),
        ),
        out_specs=(
            P("tp", KV),
            P("tp", None, KV, None, None),
            P("tp", None, KV),
            P("tp", None, KV),
        ),
        check_vma=False,
    )
```
